32 devices in a mesh: sp: 8 (over z, x), tp: 4 (over y, core).
Axes of the slice: x: 2, y: 2, z: 4, core: 2. Of those that a mesh axis runs over, the one named last changes fastest.
Arguments:
- cotangent: bfloat16 [1536, 2048], P('sp'), may hold values from -8 to 8
- residual: bfloat16 [1536, 2048], P('sp'), may hold values from -6 to 6
- norm_gain: float32 [2048], replicated, may hold values from 0.1 to 1.9
- route_ids: int32 [1536, 2], P('sp'), may hold values from 0 to 7, all different within a row; in each aligned block of 192 rows (0 to 191, 192 to 383, ...) at most 96 rows name the same one
- route_weights: float32 [1536, 2], P('sp'), may hold values from 0.1 to 1
- expert_gate: bfloat16 [8, 2048, 1024], P('sp', None, 'tp'), may hold values from -0.125 to 0.125
- expert_up: bfloat16 [8, 2048, 1024], P('sp', None, 'tp'), may hold values from -0.125 to 0.125
- expert_down: bfloat16 [8, 1024, 2048], P('sp', 'tp'), may hold values from -0.1875 to 0.1875
- out_proj: bfloat16 [2048, 1024], P(None, 'tp'), may hold values from -0.1875 to 0.1875
- conv_out: bfloat16 [1536, 1024], P('sp', 'tp'), may hold values from -6 to 6, as said below
- branch_gate: bfloat16 [1536, 1024], P('sp', 'tp'), may hold values from -6 to 6
- prev_state: bfloat16 [1536, 1024], P('sp', 'tp'), may hold values from -6 to 6
- decay_param: float32 [1024], P('tp'), as said below
- rate_map: bfloat16 [16, 64, 64], P('tp'), may hold values from -0.75 to 0.75
- input_map: bfloat16 [16, 64, 64], P('tp'), may hold values from -0.75 to 0.75
Outputs:
- grad_gate: float32 [8, 2048, 1024], P('sp', None, 'tp')
- grad_up: float32 [8, 2048, 1024], P('sp', None, 'tp')
- grad_down: float32 [8, 1024, 2048], P('sp', 'tp')
- grad_out_proj: float32 [2048, 1024], P('sp', 'tp')
- grad_conv_out: float32 [1536, 1024], P('sp', 'tp')
- grad_branch_gate: float32 [1536, 1024], P('sp', 'tp')
The draws below stay inside these ranges and needn't reach their ends.
Inputs may be any that keep to these rules, and one draw needn't show every extreme that they name: `route_ids`: within the rows of one device (aligned blocks of 192 rows) no expert is named by more than 96 rows, a bound that some block reaches; the two ids of a row differ. `conv_out`: every entry is a finite value between -6 and 6. `decay_param`: every channel's decay parameter is at least 4.
All inputs are finite; a program needn't handle non-finite values.
Results may differ from the reference program's by a relative error of at most 0.0095.
Values may be sent and summed in bfloat16 or wider, within the bound.
A program may use at most 128 MiB of HBM per device.

```python
import math
import jax
import jax.numpy as jnp
import numpy as np
from jax import lax

D = 2048
FF = 1024
W = 1024
LRU_BLOCK = 64
TOK_DEV = 192
EXPERTS = 8
CAP = 96
TOKENS = 1536
FF_PART = 256
BLOCKS = 16
N_SP = 8
N_TP = 4


def draw_conv_out(key, part):
    noise_key, offset_key = jax.random.split(key, 2)
    offsets = jax.random.uniform(offset_key, (TOKENS // 64,), jnp.float32, -1.5, 1.5)
    shifts = jnp.repeat(offsets, 64)[:, None]
    base_values = jax.random.normal(noise_key, (TOKENS, W), jnp.float32)
    return jnp.clip(base_values + shifts, -6.0, 6.0).astype(jnp.bfloat16)


def draw_decay_param(key, part):
    pick_key, slow_key, fast_key = jax.random.split(key, 3)
    chooser = jax.random.uniform(pick_key, (W,), jnp.float32)
    slow_values = jnp.log(TOKENS * 1.0) + jax.random.uniform(slow_key, (W,), jnp.float32, 1.5, 3.0)
    fast_values = jax.random.uniform(fast_key, (W,), jnp.float32, 4.8, 6.0)
    slow_share = 0.5
    return jnp.where(chooser < slow_share, slow_values, fast_values).astype(jnp.float32)


def spiked(drawn, own_key, source, target, shards_of, factor):
    def block_of(position):
        return (jnp.arange(drawn.shape[position]) // (drawn.shape[position] // shards_of)).reshape((-1,) + (1,) * (drawn.ndim - 1 - position))

    near = jax.random.permutation(own_key, shards_of)[block_of(target)]
    second = (block_of(target) + shards_of // 2) % shards_of
    return jnp.where((block_of(source) == near) | (block_of(source) == second), factor * drawn, drawn)


def block_scale(own_key, dims, cuts, smallest, high):
    level = 1.0
    for axis_at, shards_of in cuts:
        heights = jax.random.uniform(jax.random.fold_in(jax.random.fold_in(own_key, 6), axis_at), (shards_of,), jnp.float32, smallest / len(cuts), high / len(cuts))
        level = level * jnp.repeat(jnp.exp(heights), dims[axis_at] // shards_of).reshape((-1,) + (1,) * (len(dims) - 1 - axis_at))
    return level


def assign_block(own_key, own, number, rows, number_of, top, limit, skew):
    order = jax.random.permutation(own_key, number_of)
    crowded, common = portions_of(number_of, rows * top, limit, skew, True), portions_of(number_of, rows * top, limit, skew, False)
    places = jnp.arange(number_of)

    def named(sizes, rotation):
        used = int((sizes > 0).sum())
        fixed = max(1, used // 4)
        moved = fixed + (places - fixed + rotation * (used - fixed)) % max(1, number_of - fixed)
        return jnp.zeros((number_of,), jnp.int32).at[order[jnp.where(places < fixed, places, moved)]].set(jnp.asarray(sizes, jnp.int32))

    sizes = jnp.where(number % 4 == 0, named(crowded, number // 4), named(common, number - number // 4 - 1))
    mixed = jax.random.permutation(jax.random.fold_in(own, 3), number_of)
    giver, receiver = mixed[0:number_of // 2 * 2:2], mixed[1:number_of // 2 * 2:2]
    margin = jnp.minimum(sizes[giver] - 1, limit - sizes[receiver]) // 2
    margin = jnp.where((giver == order[0]) | (receiver == order[0]) | (sizes[receiver] == 0), 0, jnp.maximum(margin, 0))
    moved = jax.random.randint(jax.random.fold_in(own, 4), (number_of // 2,), 0, 1 << 20) % (margin + 1)
    sizes = sizes.at[giver].add(-moved).at[receiver].add(moved)
    labels = jnp.searchsorted(jnp.cumsum(sizes), jnp.arange(rows * top), side="right").astype(jnp.int32)
    listing = labels.reshape(top, rows).T
    listing = listing[jax.random.permutation(jax.random.fold_in(own, 1), rows)]
    rotation = jax.random.randint(jax.random.fold_in(own, 2), (rows, 1), 0, top)
    return jnp.take_along_axis(listing, (jnp.arange(top)[None, :] + rotation) % top, axis=1)


def portions_of(amount, total, limit, skew, full):
    portions = [(1 << 20) // math.isqrt(rank ** skew) + 1 for rank in range(1, amount + 1)]
    largest = limit if full else min(limit, max(-(-total // amount), total * portions[0] // sum(portions)))
    least = 1 if total - largest >= amount - 1 else 0
    holding, surplus = [largest] + [least] * (amount - 1), total - largest - least * (amount - 1)
    while surplus > 0:
        movable = [i for i in range(1, amount) if holding[i] < largest] or [i for i in range(1, amount) if holding[i] < limit]
        pool, left = sum([portions[i] for i in movable]), surplus
        for i in movable:
            extra = min(limit - holding[i], max(1, left * portions[i] // pool), surplus)
            holding[i] = holding[i] + extra
            surplus = surplus - extra
    return np.array(holding)


def centred(key, extent, scale, bound, shards=(), kind=jnp.bfloat16):
    loudness = block_scale(key, extent, shards, -0.22, 0.18) if shards else 1.0
    array = jax.random.normal(key, extent, jnp.float32) * scale * loudness
    return jnp.minimum(jnp.maximum(array, -bound), bound).astype(kind)


def gaussian_with(stream_key, extent, scale, limit, cuts, heavy, held_as=jnp.bfloat16):
    drawn = scale * jax.random.normal(stream_key, extent, jnp.float32)
    if cuts:
        drawn = drawn * block_scale(stream_key, extent, cuts, -0.22, 0.18)
    return jnp.clip(spiked(drawn, jax.random.fold_in(stream_key, 3), *heavy), -limit, limit).astype(held_as)


def setup_inputs(seed: int = 0) -> dict:
    streams_of = jax.random.split(jax.random.key(seed), 16)
    cotangent = gaussian_with(streams_of[0], (TOKENS, D), 1.0, 8.0, ((0, 8),), (0, 1, 8, 2.0))
    residual = centred(streams_of[1], (TOKENS, D), 1.0, 6.0, ((0, 8),))
    norm_gain = jnp.clip(1.0 + 0.18 * jax.random.normal(streams_of[2], (D,), jnp.float32), 0.1, 1.9)
    route_ids_keys = jax.random.split(jax.random.fold_in(streams_of[3], 1), TOKENS // TOK_DEV)
    route_ids_turns = jax.random.permutation(jax.random.fold_in(streams_of[3], 3), TOKENS // TOK_DEV)
    route_ids = jax.vmap(lambda own, number: assign_block(jax.random.fold_in(streams_of[3], 2), own, number, TOK_DEV, EXPERTS, 2, CAP, 1))(route_ids_keys, route_ids_turns).reshape((TOKENS, 2))
    route_weights = jnp.clip(0.1 + 0.9 * jax.random.uniform(streams_of[4], (TOKENS, 2), jnp.float32) ** block_scale(streams_of[4], (TOKENS, 2), ((0, 8),), -0.2, 0.2), 0.1, 1.0)
    expert_gate = centred(streams_of[5], (EXPERTS, D, FF), D ** -0.5, 0.125, ((0, 8), (2, 4)))
    expert_up = centred(streams_of[6], (EXPERTS, D, FF), D ** -0.5, 0.125, ((0, 8), (2, 4)))
    expert_down = centred(streams_of[7], (EXPERTS, FF, D), FF ** -0.5, 0.1875, ((0, 8), (1, 4)))
    out_proj = centred(streams_of[8], (D, W), W ** -0.5, 0.1875, ((1, 4),))
    conv_out = draw_conv_out(jax.random.fold_in(streams_of[15], 71), 0)
    branch_gate = centred(streams_of[10], (TOKENS, W), 1.0, 6.0, ((0, 8), (1, 4)))
    prev_state = centred(streams_of[11], (TOKENS, W), 1.0, 6.0, ((0, 8), (1, 4)))
    decay_param = draw_decay_param(jax.random.fold_in(streams_of[15], 71), 0)
    rate_map = centred(streams_of[13], (BLOCKS, LRU_BLOCK, LRU_BLOCK), LRU_BLOCK ** -0.5, 0.75, ((0, 4),))
    input_map = centred(streams_of[14], (BLOCKS, LRU_BLOCK, LRU_BLOCK), LRU_BLOCK ** -0.5, 0.75, ((0, 4),))
    return {"cotangent": cotangent, "residual": residual, "norm_gain": norm_gain, "route_ids": route_ids, "route_weights": route_weights, "expert_gate": expert_gate, "expert_up": expert_up, "expert_down": expert_down, "out_proj": out_proj, "conv_out": conv_out, "branch_gate": branch_gate, "prev_state": prev_state, "decay_param": decay_param, "rate_map": rate_map, "input_map": input_map}


RATE_SCALE = 8.0
NORM_EPS = 1e-06
SERIES_EDGE = 0.001

def gelu_pair(values):
    result, pullback = jax.vjp(jax.nn.gelu, values)
    return (result, pullback(jnp.ones_like(values))[0])

def gate_maps(conv_out, weights):
    rows_here = conv_out.shape[0]
    blocked = conv_out.astype(jnp.float32).reshape(rows_here, weights.shape[0], weights.shape[1])
    mapped = jnp.einsum('tbi,bij->tbj', blocked, weights.astype(jnp.float32))
    return mapped.reshape(rows_here, -1)

def gate_maps_back(grad_values, weights):
    rows_here = grad_values.shape[0]
    blocked = grad_values.reshape(rows_here, weights.shape[0], weights.shape[2])
    mapped = jnp.einsum('tbj,bij->tbi', blocked, weights.astype(jnp.float32), precision=lax.Precision.HIGHEST)
    return mapped.reshape(rows_here, -1)

def norm_slope(spread):
    tiny_side = spread < SERIES_EDGE
    denominator = jnp.where(tiny_side, 1.0, -jnp.expm1(-spread))
    series_ratio = jnp.where(tiny_side, 1.0 + 0.5 * spread, spread / denominator)
    return 0.5 * jnp.sqrt(spread * series_ratio)

def reverse_linear(factors, term_values):

    def combine(left_pair, right_pair):
        return (left_pair[0] * right_pair[0], right_pair[0] * left_pair[1] + right_pair[1])
    flipped = lax.associative_scan(combine, (jnp.flip(factors, 0), jnp.flip(term_values, 0)), axis=0)
    return jnp.flip(flipped[1], 0)

def reference(cotangent, residual, norm_gain, route_ids, route_weights, expert_gate, expert_up, expert_down, out_proj, conv_out, branch_gate, prev_state, decay_param, rate_map, input_map):
    res_values = residual.astype(jnp.float32)
    inv_rms = lax.rsqrt(lax.optimization_barrier(jnp.mean(res_values * res_values, axis=1, keepdims=True)) + NORM_EPS)
    moe_input = (res_values * inv_rms * norm_gain[None, :]).astype(jnp.bfloat16)
    scaled_cot = (route_weights[:, :, None] * cotangent.astype(jnp.float32)[:, None, :]).astype(jnp.bfloat16)
    scaled_cot = scaled_cot.reshape(2 * TOKENS, D)
    id_blocks = route_ids.reshape(N_SP, 2 * TOK_DEV)
    expert_hits = (id_blocks[:, :, None] == jnp.arange(EXPERTS, dtype=jnp.int32)[None, None, :]).astype(jnp.int32)
    earlier_hits = jnp.cumsum(expert_hits, axis=1) - expert_hits
    rank_in = lax.optimization_barrier(jnp.sum(earlier_hits * expert_hits, axis=2))
    global_slot = (id_blocks * (N_SP * CAP) + jnp.arange(N_SP, dtype=jnp.int32)[:, None] * CAP + rank_in).reshape(-1).astype(jnp.int32)
    slot_total = EXPERTS * N_SP * CAP
    assign_table = jnp.zeros((slot_total,), jnp.int32).at[global_slot].set(jnp.arange(2 * TOKENS, dtype=jnp.int32)).reshape(EXPERTS, N_SP * CAP)
    filled_table = jnp.zeros((slot_total,), jnp.int32).at[global_slot].set(1).reshape(EXPERTS, N_SP * CAP)

    def one_expert(packed):
        gate_one, up_one, down_one, assign_one, filled_one = packed
        rows_in = moe_input[assign_one // 2]
        cot_in = jnp.where(filled_one[:, None] > 0, scaled_cot[assign_one], jnp.zeros((), jnp.bfloat16))
        gate_pre = jnp.dot(rows_in, gate_one, preferred_element_type=jnp.float32)
        up_pre = jnp.dot(rows_in, up_one, preferred_element_type=jnp.float32)
        gate_sig = jax.nn.sigmoid(gate_pre)
        gate_act = gate_pre * gate_sig
        hidden = (gate_act * up_pre).astype(jnp.bfloat16)
        d_hidden = jnp.dot(cot_in, down_one.T, preferred_element_type=jnp.float32)
        d_up = (d_hidden * gate_act).astype(jnp.bfloat16)
        d_gate = (d_hidden * up_pre * gate_sig * (1.0 + gate_pre * (1.0 - gate_sig))).astype(jnp.bfloat16)
        grad_down_one = jnp.dot(hidden.T, cot_in, preferred_element_type=jnp.float32)
        grad_gate_one = jnp.dot(rows_in.T, d_gate, preferred_element_type=jnp.float32)
        grad_up_one = jnp.dot(rows_in.T, d_up, preferred_element_type=jnp.float32)
        rows_count = rows_in.shape[0]
        gate_blocks = d_gate.astype(jnp.float32).reshape(rows_count, N_TP, FF_PART)
        up_blocks = d_up.astype(jnp.float32).reshape(rows_count, N_TP, FF_PART)
        block_terms = jnp.einsum('rnf,dnf->nrd', gate_blocks, gate_one.astype(jnp.float32).reshape(D, N_TP, FF_PART))
        block_terms = block_terms + jnp.einsum('rnf,dnf->nrd', up_blocks, up_one.astype(jnp.float32).reshape(D, N_TP, FF_PART))
        rounded = lax.optimization_barrier(block_terms.astype(jnp.bfloat16))
        expert_back_one = lax.optimization_barrier(jnp.sum(rounded.astype(jnp.float32), axis=0)).astype(jnp.bfloat16)
        return (grad_gate_one, grad_up_one, grad_down_one, expert_back_one)
    grad_gate, grad_up, grad_down, expert_back = lax.map(one_expert, (expert_gate, expert_up, expert_down, assign_table, filled_table))
    back_rows = expert_back.reshape(slot_total, D)[global_slot].astype(jnp.float32)
    d_normed = lax.optimization_barrier(jnp.sum(back_rows.reshape(TOKENS, 2, D), axis=1))
    weighted = norm_gain[None, :] * d_normed
    cubed = inv_rms * inv_rms * inv_rms
    d_mix = (cotangent.astype(jnp.float32) + inv_rms * weighted - res_values * cubed * lax.optimization_barrier(jnp.mean(res_values * weighted, axis=1, keepdims=True))).astype(jnp.bfloat16)
    rate_gate = jax.nn.sigmoid(gate_maps(conv_out, rate_map))
    input_gate = jax.nn.sigmoid(gate_maps(conv_out, input_map))
    soft_decay = jax.nn.softplus(-decay_param)
    log_keep = -RATE_SCALE * rate_gate * soft_decay[None, :]
    keep_rate = jnp.exp(log_keep)
    spread = -2.0 * log_keep
    norm_term = jnp.sqrt(-jnp.expm1(-spread))
    conv_values = conv_out.astype(jnp.float32)
    prev_values = prev_state.astype(jnp.float32)
    state_now = keep_rate * prev_values + norm_term * input_gate * conv_values
    gelu_value, gelu_slope = gelu_pair(branch_gate.astype(jnp.float32))
    branch_out = (state_now * gelu_value).astype(jnp.bfloat16)
    grad_out_proj = lax.dot_general(d_mix, branch_out, (((0,), (0,)), ((), ())), preferred_element_type=jnp.float32)
    d_branch = jnp.dot(d_mix, out_proj, preferred_element_type=jnp.float32)
    next_keep = jnp.concatenate([keep_rate[1:], jnp.zeros_like(keep_rate[:1])], axis=0)
    state_grad = reverse_linear(next_keep, d_branch * gelu_value)
    grad_branch_gate = d_branch * state_now * gelu_slope
    keep_grad = state_grad * prev_values * keep_rate
    inner_input = input_gate * conv_values
    rate_back = keep_grad * (-RATE_SCALE * soft_decay[None, :]) * rate_gate * (1.0 - rate_gate)
    rate_back = rate_back + state_grad * inner_input * keep_rate * keep_rate * (1.0 - rate_gate) * norm_slope(spread)
    input_back = state_grad * norm_term * conv_values * input_gate * (1.0 - input_gate)
    grad_conv_out = state_grad * norm_term * input_gate + gate_maps_back(rate_back, rate_map) + gate_maps_back(input_back, input_map)
    return (grad_gate, grad_up, grad_down, grad_out_proj, grad_conv_out, grad_branch_gate)
```

```python
import functools

import jax
import jax.numpy as jnp
from jax import lax
from jax.sharding import PartitionSpec as P
from jax.experimental import pallas as pl
from jax.experimental.pallas import tpu as pltpu

RATE_SCALE = 8.0
NORM_EPS = 1e-06
SERIES_EDGE = 0.001
MESH = pl.DeviceIdType.MESH


def my_place(tp_count):
    s = lax.axis_index("sp")
    t = lax.axis_index("tp")
    beside = t + 1 - 2 * lax.rem(t, 2)
    across = lax.rem(t + tp_count // 2, tp_count)
    return s, t, beside, across


def greet(sp_count, s, t, beside, across):
    barrier = pltpu.get_barrier_semaphore()
    for other in (beside, across):
        pl.semaphore_signal(barrier, inc=1, device_id=(s, other), device_id_type=MESH)

    def one(i, carry):
        pl.semaphore_signal(
            barrier, inc=1, device_id=(lax.rem(s + i, sp_count), t), device_id_type=MESH
        )
        return carry

    lax.fori_loop(1, sp_count, one, 0)
    pl.semaphore_wait(barrier, sp_count + 1)


def remote(src, dst, send_sem, recv_sem, device):
    return pltpu.make_async_remote_copy(
        src_ref=src,
        dst_ref=dst,
        send_sem=send_sem,
        recv_sem=recv_sem,
        device_id=device,
        device_id_type=MESH,
    )


def spread_kernel(sp_count, tp_count, count, by_cols, has_small, *refs):
    sends = refs[:count]
    refs = refs[count:]
    if has_small:
        small, refs = refs[0], refs[1:]
    outs = refs[:count]
    refs = refs[count:]
    if has_small:
        small_out, refs = refs[0], refs[1:]
    local_sem, send_sem, recv_sem = refs[:3]
    s, t, beside, across = my_place(tp_count)
    facing = lax.rem(beside + tp_count // 2, tp_count)

    def view(a, source, q):
        rows, cols = sends[a].shape[1:]
        if by_cols:
            return outs[a].at[source, :, pl.ds(pl.multiple_of(q * cols, cols), cols)]
        return outs[a].at[source, pl.ds(pl.multiple_of(q * rows, rows), rows), :]

    def first(a, i):
        target = lax.rem(s + i, sp_count)
        return remote(
            sends[a].at[target],
            view(a, s, t),
            send_sem.at[0, a, i],
            recv_sem.at[0, a, i],
            (target, t),
        )

    def passed(kind, a, i, q, to):
        source = lax.rem(s + sp_count - i, sp_count)
        block = view(a, source, q)
        return remote(block, block, send_sem.at[kind, a, i], recv_sem.at[kind, a, i], (s, to))

    def little(i):
        small_send, small_recv = refs[4:6]
        return remote(
            small,
            small_out.at[s],
            small_send.at[i],
            small_recv.at[i],
            (lax.rem(s + i, sp_count), t),
        )

    greet(sp_count, s, t, beside, across)
    if has_small:
        own_small = pltpu.make_async_copy(small, small_out.at[s], refs[3].at[0])
        own_small.start()

        def start_little(i, carry):
            little(i).start()
            return carry

        lax.fori_loop(1, sp_count, start_little, 0)
    own = [
        pltpu.make_async_copy(sends[a].at[s], view(a, s, t), local_sem.at[a])
        for a in range(count)
    ]
    for copy in own:
        copy.start()

    def start_first(i, carry):
        for a in range(count):
            first(a, i).start()
        return carry

    lax.fori_loop(1, sp_count, start_first, 0)

    def pass_on(i):
        for a in range(count):
            passed(1, a, i, t, across).start()
            passed(2, a, i, t, beside).start()

    def pass_back(i):
        for a in range(count):
            passed(1, a, i, across, across).wait_recv()
            passed(3, a, i, across, beside).start()

    for copy in own:
        copy.wait()
    pass_on(0)

    def landed(i):
        for a in range(count):
            source = lax.rem(s + sp_count - i, sp_count)
            remote(
                sends[a].at[source],
                view(a, source, t),
                send_sem.at[0, a, i],
                recv_sem.at[0, a, i],
                (source, t),
            ).wait_recv()

    landed(1)
    pass_on(1)

    def middle(i, carry):
        landed(i)
        pass_on(i)
        pass_back(i - 2)
        return carry

    lax.fori_loop(2, sp_count, middle, 0)
    pass_back(sp_count - 2)
    pass_back(sp_count - 1)

    def finish(i, carry):
        for a in range(count):
            passed(2, a, i, beside, beside).wait_recv()
            passed(3, a, i, facing, beside).wait_recv()
            passed(1, a, i, t, across).wait_send()
            passed(2, a, i, t, beside).wait_send()
            passed(3, a, i, across, beside).wait_send()
        return carry

    lax.fori_loop(0, sp_count, finish, 0)

    def finish_first(i, carry):
        for a in range(count):
            first(a, i).wait_send()
        if has_small:
            little(i).wait()
        return carry

    lax.fori_loop(1, sp_count, finish_first, 0)
    if has_small:
        own_small.wait()


def spread(sp_count, tp_count, sends, by_cols, small, number):
    outs = []
    for a in sends:
        _, rows, cols = a.shape
        shape = (sp_count, rows, tp_count * cols) if by_cols else (sp_count, tp_count * rows, cols)
        outs.append(jax.ShapeDtypeStruct(shape, a.dtype))
    count = len(sends)
    operands = list(sends)
    sems = [
        pltpu.SemaphoreType.DMA((count,)),
        pltpu.SemaphoreType.DMA((4, count, sp_count)),
        pltpu.SemaphoreType.DMA((4, count, sp_count)),
    ]
    if small is not None:
        operands.append(small)
        outs.append(jax.ShapeDtypeStruct((sp_count,) + small.shape, small.dtype))
        sems += [
            pltpu.SemaphoreType.DMA((1,)),
            pltpu.SemaphoreType.DMA((sp_count,)),
            pltpu.SemaphoreType.DMA((sp_count,)),
        ]
    body = functools.partial(spread_kernel, sp_count, tp_count, count, by_cols, small is not None)
    return pl.pallas_call(
        body,
        out_shape=outs,
        in_specs=[pl.BlockSpec(memory_space=pl.ANY)] * len(operands),
        out_specs=[pl.BlockSpec(memory_space=pl.ANY)] * len(outs),
        scratch_shapes=sems,
        compiler_params=pltpu.CompilerParams(collective_id=number, has_side_effects=True),
        cost_estimate=pl.CostEstimate(flops=0, bytes_accessed=40_000_000, transcendentals=0),
    )(*operands)


def return_kernel(
    sp_count,
    tp_count,
    part,
    pick,
    branch,
    full,
    branch_all,
    from_beside,
    to_across,
    from_across,
    mine,
    leaving,
    arrived,
    quarter,
    send_sem,
    recv_sem,
    branch_send,
    branch_recv,
    last_send,
    last_recv,
    local_sem,
):
    s, t, beside, across = my_place(tp_count)
    facing = lax.rem(beside + tp_count // 2, tp_count)
    width = quarter.shape[1]
    half = sp_count // 2
    s_twin = s + 1 - 2 * lax.rem(s, 2)

    def cols(q):
        return pl.ds(pl.multiple_of(q * width, width), width)

    def place(i):
        return lax.rem(s + i + 1, sp_count)

    def to_beside(i, k):
        q = beside if k == 0 else facing
        return remote(
            part.at[place(i), :, cols(q)],
            from_beside.at[k, place(i)],
            send_sem.at[k, i],
            recv_sem.at[k, i],
            (s, beside),
        )

    def crossing(i):
        return remote(
            to_across.at[place(i)],
            from_across.at[place(i)],
            send_sem.at[2, i],
            recv_sem.at[2, i],
            (s, across),
        )

    def homeward(i):
        return remote(
            leaving.at[place(i)],
            arrived.at[s],
            send_sem.at[3, i],
            recv_sem.at[3, i],
            (place(i), t),
        )

    def branch_out_copy(j):
        return remote(
            branch,
            branch_all.at[s],
            branch_send.at[0, j],
            branch_recv.at[0, j],
            (lax.rem(s + 2 * j, sp_count), t),
        )

    def branch_twin(j):
        block = branch_all.at[lax.rem(s + sp_count - 2 * j, sp_count)]
        return remote(block, block, branch_send.at[1, j], branch_recv.at[1, j], (s_twin, t))

    greet(sp_count, s, t, beside, across)

    def start_beside(i, carry):
        to_beside(i, 1).start()
        to_beside(i, 0).start()
        return carry

    lax.fori_loop(0, sp_count, start_beside, 0)
    own_branch = pltpu.make_async_copy(branch, branch_all.at[s], local_sem.at[0])
    own_branch.start()

    def start_branch(j, carry):
        branch_out_copy(j).start()
        return carry

    lax.fori_loop(1, half, start_branch, 0)

    def cross(i):
        to_beside(i, 1).wait_recv()
        at = place(i)
        total = part[at, :, cols(across)].astype(jnp.float32) + from_beside[1, at].astype(
            jnp.float32
        )
        to_across[at] = total.astype(jnp.bfloat16)
        crossing(i).start()
        to_beside(i, 0).wait_recv()
        mine[at] = part[at, :, cols(t)].astype(jnp.float32) + from_beside[0, at].astype(
            jnp.float32
        )

    def total_of(i):
        crossing(i).wait_recv()
        at = place(i)
        return (mine[at] + from_across[at].astype(jnp.float32)).astype(jnp.bfloat16)

    def leave(i):
        leaving[place(i)] = total_of(i)
        homeward(i).start()

    cross(0)
    cross(1)

    def middle(i, carry):
        cross(i)
        leave(i - 2)
        return carry

    lax.fori_loop(2, sp_count, middle, 0)
    own_branch.wait()
    branch_twin(0).start()
    leave(sp_count - 2)
    arrived[s] = total_of(sp_count - 1)

    def pass_branch(j, carry):
        branch_out_copy(j).wait_recv()
        branch_twin(j).start()
        return carry

    lax.fori_loop(1, half, pass_branch, 0)

    quarter_sum = jnp.dot(pick[s], arrived[s], preferred_element_type=jnp.float32)

    def add_in(i, total):
        source = lax.rem(s + 2 * sp_count - i - 1, sp_count)
        remote(
            leaving.at[source],
            arrived.at[source],
            send_sem.at[3, i],
            recv_sem.at[3, i],
            (source, t),
        ).wait_recv()
        return total + jnp.dot(pick[source], arrived[source], preferred_element_type=jnp.float32)

    quarter_sum = lax.fori_loop(0, sp_count - 1, add_in, quarter_sum)
    quarter[...] = quarter_sum.astype(jnp.bfloat16)

    def gathered(kind, source, q, to):
        return remote(
            source, full.at[:, cols(q)], last_send.at[kind], last_recv.at[kind], (s, to)
        )

    own_quarter = pltpu.make_async_copy(quarter, full.at[:, cols(t)], local_sem.at[1])
    gathered(0, quarter, t, across).start()
    gathered(1, quarter, t, beside).start()
    own_quarter.start()
    gathered(0, quarter, across, across).wait_recv()
    gathered(2, full.at[:, cols(across)], across, beside).start()

    def finish(i, carry):
        to_beside(i, 0).wait_send()
        to_beside(i, 1).wait_send()
        crossing(i).wait_send()
        return carry

    lax.fori_loop(0, sp_count, finish, 0)

    def finish_home(i, carry):
        homeward(i).wait_send()
        return carry

    lax.fori_loop(0, sp_count - 1, finish_home, 0)

    def finish_branch(j, carry):
        branch_out_copy(j).wait_send()
        branch_twin(j).wait()
        return carry

    lax.fori_loop(1, half, finish_branch, 0)
    branch_twin(0).wait()
    own_quarter.wait()
    gathered(1, quarter, beside, beside).wait_recv()
    gathered(2, full.at[:, cols(facing)], facing, beside).wait_recv()
    gathered(0, quarter, t, across).wait_send()
    gathered(1, quarter, t, beside).wait_send()
    gathered(2, full.at[:, cols(across)], across, beside).wait_send()


def give_back(sp_count, tp_count, part, pick, branch, number):
    cap, model_width = part.shape[1:]
    width = model_width // tp_count
    rows = branch.shape[0]
    blocks = (sp_count, cap, width)
    return pl.pallas_call(
        functools.partial(return_kernel, sp_count, tp_count),
        out_shape=[
            jax.ShapeDtypeStruct((rows, model_width), jnp.bfloat16),
            jax.ShapeDtypeStruct((sp_count,) + branch.shape, branch.dtype),
        ],
        in_specs=[
            pl.BlockSpec(memory_space=pltpu.VMEM),
            pl.BlockSpec(memory_space=pltpu.VMEM),
            pl.BlockSpec(memory_space=pl.ANY),
        ],
        out_specs=[pl.BlockSpec(memory_space=pl.ANY)] * 2,
        scratch_shapes=[
            pltpu.VMEM((2,) + blocks, jnp.bfloat16),
            pltpu.VMEM(blocks, jnp.bfloat16),
            pltpu.VMEM(blocks, jnp.bfloat16),
            pltpu.VMEM(blocks, jnp.float32),
            pltpu.VMEM(blocks, jnp.bfloat16),
            pltpu.VMEM(blocks, jnp.bfloat16),
            pltpu.VMEM((rows, width), jnp.bfloat16),
            pltpu.SemaphoreType.DMA((4, sp_count)),
            pltpu.SemaphoreType.DMA((4, sp_count)),
            pltpu.SemaphoreType.DMA((2, sp_count // 2)),
            pltpu.SemaphoreType.DMA((2, sp_count // 2)),
            pltpu.SemaphoreType.DMA((3,)),
            pltpu.SemaphoreType.DMA((3,)),
            pltpu.SemaphoreType.DMA((2,)),
        ],
        compiler_params=pltpu.CompilerParams(collective_id=number, has_side_effects=True),
        cost_estimate=pl.CostEstimate(flops=0, bytes_accessed=40_000_000, transcendentals=0),
    )(part, pick, branch)


def gelu_pair(values):
    result, pullback = jax.vjp(jax.nn.gelu, values)
    return (result, pullback(jnp.ones_like(values))[0])


def gate_maps(conv_out, weights):
    rows_here = conv_out.shape[0]
    blocked = conv_out.reshape(rows_here, weights.shape[0], weights.shape[1])
    mapped = jnp.einsum("tbi,bij->tbj", blocked, weights, preferred_element_type=jnp.float32)
    return mapped.reshape(rows_here, -1)


def gate_maps_back(grad_values, weights):
    rows_here = grad_values.shape[0]
    blocked = grad_values.reshape(rows_here, weights.shape[0], weights.shape[2])
    mapped = jnp.einsum(
        "tbj,bij->tbi", blocked, weights.astype(jnp.float32), precision=lax.Precision.HIGHEST
    )
    return mapped.reshape(rows_here, -1)


def norm_slope(spread):
    tiny_side = spread < SERIES_EDGE
    denominator = jnp.where(tiny_side, 1.0, -jnp.expm1(-spread))
    series_ratio = jnp.where(tiny_side, 1.0 + 0.5 * spread, spread / denominator)
    return 0.5 * jnp.sqrt(spread * series_ratio)


def reverse_linear(factors, term_values):

    def combine(left_pair, right_pair):
        return (left_pair[0] * right_pair[0], right_pair[0] * left_pair[1] + right_pair[1])

    flipped = lax.associative_scan(
        combine, (jnp.flip(factors, 0), jnp.flip(term_values, 0)), axis=0
    )
    return jnp.flip(flipped[1], 0)


def per_device(
    cotangent,
    residual,
    norm_gain,
    route_ids,
    route_weights,
    expert_gate,
    expert_up,
    expert_down,
    out_proj,
    conv_out,
    branch_gate,
    prev_state,
    decay_param,
    rate_map,
    input_map,
):
    tok_rows, model_width = residual.shape
    sp_count = lax.axis_size("sp")
    tp_count = lax.axis_size("tp")
    experts_all = expert_gate.shape[0] * sp_count
    capacity = 4 * tok_rows // experts_all
    slot_total = experts_all * capacity
    part_cols = model_width // tp_count
    col_start = lax.axis_index("tp") * part_cols
    res_values = residual.astype(jnp.float32)
    inv_rms = lax.rsqrt(jnp.mean(res_values * res_values, axis=1, keepdims=True) + NORM_EPS)

    def my_cols(values):
        return lax.dynamic_slice_in_dim(values, col_start, part_cols, values.ndim - 1)

    moe_part = (
        my_cols(residual).astype(jnp.float32) * inv_rms * my_cols(norm_gain)[None, :]
    ).astype(jnp.bfloat16)
    flat_ids = route_ids.reshape(-1)
    expert_hits = (flat_ids[:, None] == jnp.arange(experts_all, dtype=jnp.int32)[None, :]).astype(
        jnp.int32
    )
    earlier_hits = jnp.cumsum(expert_hits, axis=0) - expert_hits
    slot_pos = flat_ids * capacity + jnp.sum(earlier_hits * expert_hits, axis=1)
    slot_pair = slot_pos.reshape(tok_rows, 2)
    slots = jnp.arange(slot_total, dtype=jnp.int32)
    hit_first = slots[:, None] == slot_pair[None, :, 0]
    hit_second = slots[:, None] == slot_pair[None, :, 1]
    slot_weight = jnp.sum(
        jnp.where(hit_first, route_weights[None, :, 0], 0.0)
        + jnp.where(hit_second, route_weights[None, :, 1], 0.0),
        axis=1,
        keepdims=True,
    )
    choose = (hit_first | hit_second).astype(jnp.bfloat16)
    rows_part = jnp.dot(choose, moe_part, preferred_element_type=jnp.float32).astype(jnp.bfloat16)
    cot_part = (
        jnp.dot(choose, my_cols(cotangent), preferred_element_type=jnp.float32) * slot_weight
    ).astype(jnp.bfloat16)
    block_rows = slot_total // sp_count
    rows_in, cot_in = spread(
        sp_count,
        tp_count,
        (
            rows_part.reshape(sp_count, block_rows, part_cols),
            cot_part.reshape(sp_count, block_rows, part_cols),
        ),
        True,
        None,
        1,
    )
    rows_in = rows_in.reshape(slot_total, model_width)
    cot_in = cot_in.reshape(slot_total, model_width)
    gate_w, up_w, down_w = expert_gate[0], expert_up[0], expert_down[0]
    gate_pre = jnp.dot(rows_in, gate_w, preferred_element_type=jnp.float32)
    up_pre = jnp.dot(rows_in, up_w, preferred_element_type=jnp.float32)
    gate_sig = jax.nn.sigmoid(gate_pre)
    gate_act = gate_pre * gate_sig
    hidden = (gate_act * up_pre).astype(jnp.bfloat16)
    d_hidden = jnp.einsum("rd,fd->rf", cot_in, down_w, preferred_element_type=jnp.float32)
    d_up = (d_hidden * gate_act).astype(jnp.bfloat16)
    d_gate = (d_hidden * up_pre * gate_sig * (1.0 + gate_pre * (1.0 - gate_sig))).astype(
        jnp.bfloat16
    )
    grad_down = jnp.einsum("rf,rd->fd", hidden, cot_in, preferred_element_type=jnp.float32)[None]
    grad_gate = jnp.einsum("rd,rf->df", rows_in, d_gate, preferred_element_type=jnp.float32)[None]
    grad_up = jnp.einsum("rd,rf->df", rows_in, d_up, preferred_element_type=jnp.float32)[None]
    back_terms = jnp.einsum("rf,df->rd", d_gate, gate_w, preferred_element_type=jnp.float32)
    back_terms = back_terms + jnp.einsum("rf,df->rd", d_up, up_w, preferred_element_type=jnp.float32)
    back_terms = back_terms.astype(jnp.bfloat16).reshape(sp_count, block_rows, model_width)
    rate_gate = jax.nn.sigmoid(gate_maps(conv_out, rate_map))
    input_gate = jax.nn.sigmoid(gate_maps(conv_out, input_map))
    soft_decay = jax.nn.softplus(-decay_param)
    log_keep = -RATE_SCALE * rate_gate * soft_decay[None, :]
    keep_rate = jnp.exp(log_keep)
    spread_values = -2.0 * log_keep
    norm_term = jnp.sqrt(-jnp.expm1(-spread_values))
    conv_values = conv_out.astype(jnp.float32)
    prev_values = prev_state.astype(jnp.float32)
    state_now = keep_rate * prev_values + norm_term * input_gate * conv_values
    gelu_value, gelu_slope = gelu_pair(branch_gate.astype(jnp.float32))
    branch_out = (state_now * gelu_value).astype(jnp.bfloat16)
    slot_grid = slots.reshape(sp_count, 1, block_rows)
    pick = (
        (slot_grid == slot_pair[None, :, 0:1]) | (slot_grid == slot_pair[None, :, 1:2])
    ).astype(jnp.bfloat16)
    d_normed, branch_all = give_back(sp_count, tp_count, back_terms, pick, branch_out, 2)
    weighted = norm_gain[None, :] * d_normed.astype(jnp.float32)
    cubed = inv_rms * inv_rms * inv_rms
    d_mix = (
        cotangent.astype(jnp.float32)
        + inv_rms * weighted
        - res_values * cubed * jnp.mean(res_values * weighted, axis=1, keepdims=True)
    ).astype(jnp.bfloat16)
    d_branch = jnp.dot(d_mix, out_proj, preferred_element_type=jnp.float32)
    next_keep = jnp.concatenate([keep_rate[1:], jnp.zeros_like(keep_rate[:1])], axis=0)
    local_grad = reverse_linear(next_keep, d_branch * gelu_value)
    next_log = jnp.concatenate([log_keep[1:], jnp.zeros_like(log_keep[:1])], axis=0)
    tail_keep = jnp.exp(jnp.flip(jnp.cumsum(jnp.flip(next_log, 0), axis=0), 0))
    block_keep = jnp.exp(jnp.sum(log_keep, axis=0))
    head_term = keep_rate[0] * local_grad[0]
    channels = block_keep.shape[0]
    small = jnp.concatenate(
        [block_keep[None], head_term[None], jnp.zeros((6, channels), jnp.float32)], axis=0
    )
    share_rows = tok_rows // tp_count
    out_rows = model_width // sp_count
    mix_share = lax.dynamic_slice_in_dim(d_mix, lax.axis_index("tp") * share_rows, share_rows, 0)
    mix_share = jnp.transpose(mix_share.reshape(share_rows, sp_count, out_rows), (1, 0, 2))
    mix_cols, small_all = spread(sp_count, tp_count, (mix_share,), False, small, 3)
    grad_out_proj = lax.dot_general(
        mix_cols.reshape(sp_count * tok_rows, out_rows),
        branch_all.reshape(sp_count * tok_rows, channels),
        (((0,), (0,)), ((), ())),
        preferred_element_type=jnp.float32,
    )
    place = lax.axis_index("sp")
    carried = jnp.zeros((channels,), jnp.float32)
    for source in range(sp_count - 1, 0, -1):
        carried = jnp.where(
            source > place, small_all[source, 1] + small_all[source, 0] * carried, carried
        )
    state_grad = local_grad + tail_keep * carried[None, :]
    grad_branch_gate = d_branch * state_now * gelu_slope
    keep_grad = state_grad * prev_values * keep_rate
    inner_input = input_gate * conv_values
    rate_back = keep_grad * (-RATE_SCALE * soft_decay[None, :]) * rate_gate * (1.0 - rate_gate)
    rate_back = rate_back + state_grad * inner_input * keep_rate * keep_rate * (
        1.0 - rate_gate
    ) * norm_slope(spread_values)
    input_back = state_grad * norm_term * conv_values * input_gate * (1.0 - input_gate)
    grad_conv_out = (
        state_grad * norm_term * input_gate
        + gate_maps_back(rate_back, rate_map)
        + gate_maps_back(input_back, input_map)
    )
    return (grad_gate, grad_up, grad_down, grad_out_proj, grad_conv_out, grad_branch_gate)


def solution(mesh):
    in_specs = (
        P("sp", None),
        P("sp", None),
        P(),
        P("sp", None),
        P("sp", None),
        P("sp", None, "tp"),
        P("sp", None, "tp"),
        P("sp", "tp", None),
        P(None, "tp"),
        P("sp", "tp"),
        P("sp", "tp"),
        P("sp", "tp"),
        P("tp"),
        P("tp", None, None),
        P("tp", None, None),
    )
    out_specs = (
        P("sp", None, "tp"),
        P("sp", None, "tp"),
        P("sp", "tp", None),
        P("sp", "tp"),
        P("sp", "tp"),
        P("sp", "tp"),
    )
    return jax.shard_map(
        per_device, mesh=mesh, in_specs=in_specs, out_specs=out_specs, check_vma=False
    )
```

```python
import functools

import jax
import jax.numpy as jnp
from jax import lax
from jax.sharding import PartitionSpec as P
from jax.experimental import pallas as pl
from jax.experimental.pallas import tpu as pltpu

RATE_SCALE = 8.0
NORM_EPS = 1e-06
SERIES_EDGE = 0.001
MESH = pl.DeviceIdType.MESH


def my_place(tp_count):
    s = lax.axis_index("sp")
    t = lax.axis_index("tp")
    beside = t + 1 - 2 * lax.rem(t, 2)
    across = lax.rem(t + tp_count // 2, tp_count)
    return s, t, beside, across


def hail(sp_count, s, t, beside, across):
    barrier = pltpu.get_barrier_semaphore()
    for other in (beside, across):
        pl.semaphore_signal(barrier, inc=1, device_id=(s, other), device_id_type=MESH)

    def one(i, carry):
        pl.semaphore_signal(
            barrier, inc=1, device_id=(lax.rem(s + i, sp_count), t), device_id_type=MESH
        )
        return carry

    lax.fori_loop(1, sp_count, one, 0)


def await_hails(sp_count):
    pl.semaphore_wait(pltpu.get_barrier_semaphore(), sp_count + 1)


def greet(sp_count, s, t, beside, across):
    hail(sp_count, s, t, beside, across)
    await_hails(sp_count)


def remote(src, dst, send_sem, recv_sem, device):
    return pltpu.make_async_remote_copy(
        src_ref=src,
        dst_ref=dst,
        send_sem=send_sem,
        recv_sem=recv_sem,
        device_id=device,
        device_id_type=MESH,
    )


def spreading(sp_count, tp_count, sends, outs, by_cols, local_sem, send_sem, recv_sem):
    s, t, beside, across = my_place(tp_count)
    facing = lax.rem(beside + tp_count // 2, tp_count)
    count = len(sends)

    def view(a, source, q):
        rows, cols = sends[a].shape[1:]
        if by_cols:
            return outs[a].at[source, :, pl.ds(pl.multiple_of(q * cols, cols), cols)]
        return outs[a].at[source, pl.ds(pl.multiple_of(q * rows, rows), rows), :]

    def first(a, i):
        target = lax.rem(s + i, sp_count)
        return remote(
            sends[a].at[target],
            view(a, s, t),
            send_sem.at[0, a, i],
            recv_sem.at[0, a, i],
            (target, t),
        )

    def own(a):
        return pltpu.make_async_copy(sends[a].at[s], view(a, s, t), local_sem.at[a])

    def passed(kind, a, i, q, to):
        source = lax.rem(s + sp_count - i, sp_count)
        block = view(a, source, q)
        return remote(block, block, send_sem.at[kind, a, i], recv_sem.at[kind, a, i], (s, to))

    def pass_on(i):
        for a in range(count):
            passed(1, a, i, t, across).start()
            passed(2, a, i, t, beside).start()

    def pass_back(i):
        for a in range(count):
            passed(1, a, i, across, across).wait_recv()
            passed(3, a, i, across, beside).start()

    def landed(i):
        for a in range(count):
            source = lax.rem(s + sp_count - i, sp_count)
            remote(
                sends[a].at[source],
                view(a, source, t),
                send_sem.at[0, a, i],
                recv_sem.at[0, a, i],
                (source, t),
            ).wait_recv()

    def start(i):
        for a in range(count):
            first(a, i).start()

    def start_own():
        for a in range(count):
            own(a).start()

    def pass_own():
        for a in range(count):
            own(a).wait()
        pass_on(0)

    def relay():
        landed(1)
        pass_on(1)

        def middle(i, carry):
            landed(i)
            pass_on(i)
            pass_back(i - 2)
            return carry

        lax.fori_loop(2, sp_count, middle, 0)
        pass_back(sp_count - 2)
        pass_back(sp_count - 1)

    def finish():
        def one(i, carry):
            for a in range(count):
                passed(2, a, i, beside, beside).wait_recv()
                passed(3, a, i, facing, beside).wait_recv()
                passed(1, a, i, t, across).wait_send()
                passed(2, a, i, t, beside).wait_send()
                passed(3, a, i, across, beside).wait_send()
            return carry

        lax.fori_loop(0, sp_count, one, 0)

        def one_first(i, carry):
            for a in range(count):
                first(a, i).wait_send()
            return carry

        lax.fori_loop(1, sp_count, one_first, 0)

    return start, start_own, pass_own, relay, finish


def spread_sems(sp_count, count):
    return [
        pltpu.SemaphoreType.DMA((count,)),
        pltpu.SemaphoreType.DMA((4, count, sp_count)),
        pltpu.SemaphoreType.DMA((4, count, sp_count)),
    ]


def one_less_exp(spread):
    small = jnp.minimum(spread, 0.3)
    series = jnp.full_like(small, 1.0 / 40320.0)
    for factorial in (5040.0, 720.0, 120.0, 24.0, 6.0, 2.0, 1.0):
        series = 1.0 / factorial - small * series
    return jnp.where(spread < 0.3, small * series, 1.0 - jnp.exp(-spread))


def dispatch_kernel(
    sp_count,
    tp_count,
    res,
    cot,
    gain,
    ids,
    weights,
    conv,
    gate,
    prev,
    soft,
    maps,
    rows_out,
    cot_out,
    branch_out,
    rate_factor,
    input_factor,
    direct_factor,
    gate_factor,
    gelu_out,
    keep_out,
    send_rows,
    send_cot,
    moe_part,
    scaled_first,
    scaled_second,
    pre_values,
    local_sem,
    send_sem,
    recv_sem,
):
    s, t, beside, across = my_place(tp_count)
    hail(sp_count, s, t, beside, across)
    start, start_own, pass_own, relay, finish = spreading(
        sp_count,
        tp_count,
        (send_rows, send_cot),
        (rows_out, cot_out),
        True,
        local_sem,
        send_sem,
        recv_sem,
    )
    tok_rows = res.shape[0]
    cap, width = send_rows.shape[1:]
    cols = pl.ds(pl.multiple_of(t * width, width), width)
    res_all = res[...].astype(jnp.float32)
    inv_rms = lax.rsqrt(jnp.mean(res_all * res_all, axis=1, keepdims=True) + NORM_EPS)
    moe_part[...] = (res[:, cols].astype(jnp.float32) * inv_rms * gain[:, cols]).astype(
        jnp.bfloat16
    )
    cot_mine = cot[:, cols].astype(jnp.float32)
    scaled_first[...] = (weights[:, 0:1] * cot_mine).astype(jnp.bfloat16)
    scaled_second[...] = (weights[:, 1:2] * cot_mine).astype(jnp.bfloat16)
    experts = lax.broadcasted_iota(jnp.int32, (tok_rows, sp_count), 1)
    is_first = ids[:, 0:1] == experts
    is_second = ids[:, 1:2] == experts
    hits = (is_first | is_second).astype(jnp.float32).astype(jnp.bfloat16)
    earlier = (
        lax.broadcasted_iota(jnp.int32, (tok_rows, tok_rows), 0)
        > lax.broadcasted_iota(jnp.int32, (tok_rows, tok_rows), 1)
    )
    earlier = earlier.astype(jnp.float32).astype(jnp.bfloat16)
    ranks = jnp.dot(earlier, hits, preferred_element_type=jnp.float32)
    slot_first = jnp.sum(jnp.where(is_first, ranks, 0.0), axis=1, keepdims=True)
    slot_second = jnp.sum(jnp.where(is_second, ranks, 0.0), axis=1, keepdims=True)
    slot_first = slot_first + (ids[:, 0:1] * cap).astype(jnp.float32)
    slot_second = slot_second + (ids[:, 1:2] * cap).astype(jnp.float32)
    lanes = lax.broadcasted_iota(jnp.int32, (tok_rows, cap), 1).astype(jnp.float32)
    over_rows = (((0,), (0,)), ((), ()))

    def fill(target):
        base = (target * cap).astype(jnp.float32)
        first = jnp.where(slot_first - base == lanes, 1.0, 0.0)
        second = jnp.where(slot_second - base == lanes, 1.0, 0.0)
        send_rows[target] = lax.dot_general(
            (first + second).astype(jnp.bfloat16),
            moe_part[...],
            over_rows,
            preferred_element_type=jnp.float32,
        ).astype(jnp.bfloat16)
        from_first = lax.dot_general(
            first.astype(jnp.bfloat16),
            scaled_first[...],
            over_rows,
            preferred_element_type=jnp.float32,
        )
        from_second = lax.dot_general(
            second.astype(jnp.bfloat16),
            scaled_second[...],
            over_rows,
            preferred_element_type=jnp.float32,
        )
        send_cot[target] = (from_first + from_second).astype(jnp.bfloat16)

    fill(s)
    await_hails(sp_count)
    start_own()

    def send_one(i, carry):
        fill(lax.rem(s + i, sp_count))
        start(i)
        return carry

    lax.fori_loop(1, sp_count, send_one, 0)
    pass_own()
    channels = conv.shape[1]
    pre_values[...] = jnp.dot(conv[...], maps[...], preferred_element_type=jnp.float32)
    step = 16

    def forward(i, carry):
        rows = pl.ds(pl.multiple_of(i * step, step), step)
        rate_gate = jax.nn.sigmoid(pre_values[rows, :channels])
        input_gate = jax.nn.sigmoid(pre_values[rows, channels:])
        log_keep = -RATE_SCALE * rate_gate * soft[...]
        keep = jnp.exp(log_keep)
        spread = -2.0 * log_keep
        gone = one_less_exp(spread)
        norm_term = jnp.sqrt(gone)
        conv_values = conv[rows, :].astype(jnp.float32)
        prev_values = prev[rows, :].astype(jnp.float32)
        inner = input_gate * conv_values
        state_now = keep * prev_values + norm_term * inner
        v = gate[rows, :].astype(jnp.float32)
        root = 0.7978845608028654
        bent = jnp.tanh(root * (v + 0.044715 * v * v * v))
        gelu_value = 0.5 * v * (1.0 + bent)
        gelu_slope = 0.5 * (1.0 + bent) + 0.5 * v * (1.0 - bent * bent) * root * (
            1.0 + 3.0 * 0.044715 * v * v
        )
        tiny_side = spread < SERIES_EDGE
        series = jnp.where(tiny_side, 1.0 + 0.5 * spread, spread / jnp.where(tiny_side, 1.0, gone))
        slope = 0.5 * jnp.sqrt(spread * series)
        branch_out[rows, :] = (state_now * gelu_value).astype(jnp.bfloat16)
        rate_factor[rows, :] = prev_values * keep * (
            -RATE_SCALE * soft[...]
        ) * rate_gate * (1.0 - rate_gate) + inner * keep * keep * (1.0 - rate_gate) * slope
        input_factor[rows, :] = norm_term * conv_values * input_gate * (1.0 - input_gate)
        direct_factor[rows, :] = norm_term * input_gate
        gate_factor[rows, :] = state_now * gelu_slope
        gelu_out[rows, :] = gelu_value
        keep_out[rows, :] = keep
        return carry

    lax.fori_loop(0, tok_rows // step, forward, 0)
    relay()
    finish()


def dispatch(sp_count, tp_count, cap, operands, number):
    res, conv = operands[0], operands[5]
    tok_rows, model_width = res.shape
    width = model_width // tp_count
    wide = jax.ShapeDtypeStruct((sp_count, cap, model_width), jnp.bfloat16)
    factor = jax.ShapeDtypeStruct(conv.shape, jnp.float32)
    vmem = pl.BlockSpec(memory_space=pltpu.VMEM)
    anywhere = pl.BlockSpec(memory_space=pl.ANY)
    return pl.pallas_call(
        functools.partial(dispatch_kernel, sp_count, tp_count),
        out_shape=[wide, wide, jax.ShapeDtypeStruct(conv.shape, jnp.bfloat16)] + [factor] * 6,
        in_specs=[vmem] * len(operands),
        out_specs=[anywhere] * 2 + [vmem] * 7,
        scratch_shapes=[
            pltpu.VMEM((sp_count, cap, width), jnp.bfloat16),
            pltpu.VMEM((sp_count, cap, width), jnp.bfloat16),
            pltpu.VMEM((tok_rows, width), jnp.bfloat16),
            pltpu.VMEM((tok_rows, width), jnp.bfloat16),
            pltpu.VMEM((tok_rows, width), jnp.bfloat16),
            pltpu.VMEM((tok_rows, 2 * conv.shape[1]), jnp.float32),
        ]
        + spread_sems(sp_count, 2),
        compiler_params=pltpu.CompilerParams(collective_id=number, has_side_effects=True),
        cost_estimate=pl.CostEstimate(flops=0, bytes_accessed=40_000_000, transcendentals=0),
    )(*operands)


def tail_kernel(
    sp_count,
    tp_count,
    normed,
    res,
    cot,
    gain,
    proj,
    maps,
    rate_factor,
    input_factor,
    direct_factor,
    gate_factor,
    gelu_values,
    keep,
    mix_out,
    conv_grad,
    gate_grad,
    share,
    mix,
    small,
    small_all,
    local_sem,
    send_sem,
    recv_sem,
    small_send,
    small_recv,
):
    s, t, beside, across = my_place(tp_count)
    hail(sp_count, s, t, beside, across)
    start, start_own, pass_own, relay, finish = spreading(
        sp_count, tp_count, (share,), (mix_out,), False, local_sem, send_sem, recv_sem
    )
    tok_rows, model_width = res.shape
    share_rows, out_rows = share.shape[1:]

    def mix_rows(begin):
        rows = pl.ds(pl.multiple_of(begin, share_rows), share_rows)
        values = res[rows, :].astype(jnp.float32)
        weighted = gain[...] * normed[rows, :].astype(jnp.float32)
        inv_rms = lax.rsqrt(jnp.mean(values * values, axis=1, keepdims=True) + NORM_EPS)
        cubed = inv_rms * inv_rms * inv_rms
        slope = cubed * jnp.mean(values * weighted, axis=1, keepdims=True)
        return rows, (
            cot[rows, :].astype(jnp.float32) + inv_rms * weighted - values * slope
        ).astype(jnp.bfloat16)

    _, own_rows = mix_rows(t * share_rows)
    for j in range(sp_count):
        share[j] = own_rows[:, j * out_rows : (j + 1) * out_rows]
    await_hails(sp_count)
    start_own()

    def send_one(i, carry):
        start(i)
        return carry

    lax.fori_loop(1, sp_count, send_one, 0)

    def fill(k, carry):
        rows, values = mix_rows(k * share_rows)
        mix[rows, :] = values
        return carry

    lax.fori_loop(0, tp_count, fill, 0)
    pass_own()
    d_branch = jnp.dot(mix[...], proj[...], preferred_element_type=jnp.float32)
    gate_grad[...] = d_branch * gate_factor[...]
    at = lax.broadcasted_iota(jnp.int32, d_branch.shape, 0)
    grads = d_branch * gelu_values[...]
    keeps = jnp.where(at < tok_rows - 1, pltpu.roll(keep[...], tok_rows - 1, 0), 1.0)
    reach = 1
    while reach < tok_rows:
        inside = at < tok_rows - reach
        later_grads = jnp.where(inside, pltpu.roll(grads, tok_rows - reach, 0), 0.0)
        later_keeps = jnp.where(inside, pltpu.roll(keeps, tok_rows - reach, 0), 1.0)
        grads = grads + keeps * later_grads
        keeps = keeps * later_keeps
        reach *= 2
    small[...] = jnp.zeros_like(small)
    small[0:1, :] = keep[0:1, :] * keeps[0:1, :]
    small[1:2, :] = keep[0:1, :] * grads[0:1, :]
    small_all[s] = jnp.zeros(small.shape, jnp.float32)

    def carry_to(i):
        return remote(
            small,
            small_all.at[s],
            small_send.at[i],
            small_recv.at[i],
            (lax.rem(s + i, sp_count), t),
        )

    def send_small(i, carry):
        carry_to(i).start()
        return carry

    lax.fori_loop(1, sp_count, send_small, 0)
    relay()

    def take_small(i, carry):
        source = lax.rem(s + sp_count - i, sp_count)
        remote(
            small, small_all.at[source], small_send.at[i], small_recv.at[i], (source, t)
        ).wait_recv()
        return carry

    lax.fori_loop(1, sp_count, take_small, 0)

    def compose(turn, carried):
        source = sp_count - 1 - turn
        later = small_all[source]
        return jnp.where(source > s, later[1:2] + later[0:1] * carried, carried)

    carried = lax.fori_loop(
        0, sp_count - 1, compose, jnp.zeros((1, d_branch.shape[1]), jnp.float32)
    )
    state_grad = grads + keeps * carried
    back = jnp.concatenate(
        [state_grad * rate_factor[...], state_grad * input_factor[...]], axis=1
    )
    high = back.astype(jnp.bfloat16)
    low = (back - high.astype(jnp.float32)).astype(jnp.bfloat16)
    over_cols = (((1,), (1,)), ((), ()))
    conv_grad[...] = (
        state_grad * direct_factor[...]
        + lax.dot_general(high, maps[...], over_cols, preferred_element_type=jnp.float32)
        + lax.dot_general(low, maps[...], over_cols, preferred_element_type=jnp.float32)
    )
    finish()

    def end_small(i, carry):
        carry_to(i).wait_send()
        return carry

    lax.fori_loop(1, sp_count, end_small, 0)


def tail(sp_count, tp_count, operands, number):
    res, keep = operands[1], operands[-1]
    tok_rows, model_width = res.shape
    share_rows, out_rows = tok_rows // tp_count, model_width // sp_count
    factor = jax.ShapeDtypeStruct(keep.shape, jnp.float32)
    vmem = pl.BlockSpec(memory_space=pltpu.VMEM)
    return pl.pallas_call(
        functools.partial(tail_kernel, sp_count, tp_count),
        out_shape=[
            jax.ShapeDtypeStruct((sp_count, tok_rows, out_rows), jnp.bfloat16),
            factor,
            factor,
        ],
        in_specs=[vmem] * len(operands),
        out_specs=[pl.BlockSpec(memory_space=pl.ANY), vmem, vmem],
        scratch_shapes=[
            pltpu.VMEM((sp_count, share_rows, out_rows), jnp.bfloat16),
            pltpu.VMEM((tok_rows, model_width), jnp.bfloat16),
            pltpu.VMEM((8, keep.shape[1]), jnp.float32),
            pltpu.VMEM((sp_count, 8, keep.shape[1]), jnp.float32),
        ]
        + spread_sems(sp_count, 1)
        + [pltpu.SemaphoreType.DMA((sp_count,)), pltpu.SemaphoreType.DMA((sp_count,))],
        compiler_params=pltpu.CompilerParams(collective_id=number, has_side_effects=True),
        cost_estimate=pl.CostEstimate(flops=0, bytes_accessed=20_000_000, transcendentals=0),
    )(*operands)


def return_kernel(
    sp_count,
    tp_count,
    part,
    pick,
    branch,
    full,
    branch_all,
    from_beside,
    to_across,
    from_across,
    mine,
    leaving,
    arrived,
    quarter,
    send_sem,
    recv_sem,
    branch_send,
    branch_recv,
    last_send,
    last_recv,
    local_sem,
):
    s, t, beside, across = my_place(tp_count)
    facing = lax.rem(beside + tp_count // 2, tp_count)
    width = quarter.shape[1]
    half = sp_count // 2
    s_twin = s + 1 - 2 * lax.rem(s, 2)

    def cols(q):
        return pl.ds(pl.multiple_of(q * width, width), width)

    def place(i):
        return lax.rem(s + i + 1, sp_count)

    def to_beside(i, k):
        q = beside if k == 0 else facing
        return remote(
            part.at[place(i), :, cols(q)],
            from_beside.at[k, place(i)],
            send_sem.at[k, i],
            recv_sem.at[k, i],
            (s, beside),
        )

    def crossing(i):
        return remote(
            to_across.at[place(i)],
            from_across.at[place(i)],
            send_sem.at[2, i],
            recv_sem.at[2, i],
            (s, across),
        )

    def homeward(i):
        return remote(
            leaving.at[place(i)],
            arrived.at[s],
            send_sem.at[3, i],
            recv_sem.at[3, i],
            (place(i), t),
        )

    def branch_out_copy(j):
        return remote(
            branch,
            branch_all.at[s],
            branch_send.at[0, j],
            branch_recv.at[0, j],
            (lax.rem(s + 2 * j, sp_count), t),
        )

    def branch_twin(j):
        block = branch_all.at[lax.rem(s + sp_count - 2 * j, sp_count)]
        return remote(block, block, branch_send.at[1, j], branch_recv.at[1, j], (s_twin, t))

    greet(sp_count, s, t, beside, across)

    def start_beside(i, carry):
        to_beside(i, 1).start()
        to_beside(i, 0).start()
        return carry

    lax.fori_loop(0, sp_count, start_beside, 0)
    own_branch = pltpu.make_async_copy(branch, branch_all.at[s], local_sem.at[0])
    own_branch.start()

    def start_branch(j, carry):
        branch_out_copy(j).start()
        return carry

    lax.fori_loop(1, half, start_branch, 0)

    def cross(i):
        to_beside(i, 1).wait_recv()
        at = place(i)
        total = part[at, :, cols(across)].astype(jnp.float32) + from_beside[1, at].astype(
            jnp.float32
        )
        to_across[at] = total.astype(jnp.bfloat16)
        crossing(i).start()
        to_beside(i, 0).wait_recv()
        mine[at] = part[at, :, cols(t)].astype(jnp.float32) + from_beside[0, at].astype(
            jnp.float32
        )

    def total_of(i):
        crossing(i).wait_recv()
        at = place(i)
        return (mine[at] + from_across[at].astype(jnp.float32)).astype(jnp.bfloat16)

    def leave(i):
        leaving[place(i)] = total_of(i)
        homeward(i).start()

    cross(0)
    cross(1)

    def middle(i, carry):
        cross(i)
        leave(i - 2)
        return carry

    lax.fori_loop(2, sp_count, middle, 0)
    own_branch.wait()
    branch_twin(0).start()
    leave(sp_count - 2)
    arrived[s] = total_of(sp_count - 1)

    def pass_branch(j, carry):
        branch_out_copy(j).wait_recv()
        branch_twin(j).start()
        return carry

    lax.fori_loop(1, half, pass_branch, 0)

    quarter_sum = jnp.dot(pick[s], arrived[s], preferred_element_type=jnp.float32)

    def add_in(i, total):
        source = lax.rem(s + 2 * sp_count - i - 1, sp_count)
        remote(
            leaving.at[source],
            arrived.at[source],
            send_sem.at[3, i],
            recv_sem.at[3, i],
            (source, t),
        ).wait_recv()
        return total + jnp.dot(pick[source], arrived[source], preferred_element_type=jnp.float32)

    quarter_sum = lax.fori_loop(0, sp_count - 1, add_in, quarter_sum)
    quarter[...] = quarter_sum.astype(jnp.bfloat16)

    def gathered(kind, source, q, to):
        return remote(
            source, full.at[:, cols(q)], last_send.at[kind], last_recv.at[kind], (s, to)
        )

    own_quarter = pltpu.make_async_copy(quarter, full.at[:, cols(t)], local_sem.at[1])
    gathered(0, quarter, t, across).start()
    gathered(1, quarter, t, beside).start()
    own_quarter.start()
    gathered(0, quarter, across, across).wait_recv()
    gathered(2, full.at[:, cols(across)], across, beside).start()

    def finish(i, carry):
        to_beside(i, 0).wait_send()
        to_beside(i, 1).wait_send()
        crossing(i).wait_send()
        return carry

    lax.fori_loop(0, sp_count, finish, 0)

    def finish_home(i, carry):
        homeward(i).wait_send()
        return carry

    lax.fori_loop(0, sp_count - 1, finish_home, 0)

    def finish_branch(j, carry):
        branch_out_copy(j).wait_send()
        branch_twin(j).wait()
        return carry

    lax.fori_loop(1, half, finish_branch, 0)
    branch_twin(0).wait()
    own_quarter.wait()
    gathered(1, quarter, beside, beside).wait_recv()
    gathered(2, full.at[:, cols(facing)], facing, beside).wait_recv()
    gathered(0, quarter, t, across).wait_send()
    gathered(1, quarter, t, beside).wait_send()
    gathered(2, full.at[:, cols(across)], across, beside).wait_send()


def give_back(sp_count, tp_count, part, pick, branch, number):
    cap, model_width = part.shape[1:]
    width = model_width // tp_count
    rows = branch.shape[0]
    blocks = (sp_count, cap, width)
    return pl.pallas_call(
        functools.partial(return_kernel, sp_count, tp_count),
        out_shape=[
            jax.ShapeDtypeStruct((rows, model_width), jnp.bfloat16),
            jax.ShapeDtypeStruct((sp_count,) + branch.shape, branch.dtype),
        ],
        in_specs=[
            pl.BlockSpec(memory_space=pltpu.VMEM),
            pl.BlockSpec(memory_space=pltpu.VMEM),
            pl.BlockSpec(memory_space=pl.ANY),
        ],
        out_specs=[pl.BlockSpec(memory_space=pl.ANY)] * 2,
        scratch_shapes=[
            pltpu.VMEM((2,) + blocks, jnp.bfloat16),
            pltpu.VMEM(blocks, jnp.bfloat16),
            pltpu.VMEM(blocks, jnp.bfloat16),
            pltpu.VMEM(blocks, jnp.float32),
            pltpu.VMEM(blocks, jnp.bfloat16),
            pltpu.VMEM(blocks, jnp.bfloat16),
            pltpu.VMEM((rows, width), jnp.bfloat16),
            pltpu.SemaphoreType.DMA((4, sp_count)),
            pltpu.SemaphoreType.DMA((4, sp_count)),
            pltpu.SemaphoreType.DMA((2, sp_count // 2)),
            pltpu.SemaphoreType.DMA((2, sp_count // 2)),
            pltpu.SemaphoreType.DMA((3,)),
            pltpu.SemaphoreType.DMA((3,)),
            pltpu.SemaphoreType.DMA((2,)),
        ],
        compiler_params=pltpu.CompilerParams(collective_id=number, has_side_effects=True),
        cost_estimate=pl.CostEstimate(flops=0, bytes_accessed=40_000_000, transcendentals=0),
    )(part, pick, branch)


def per_device(
    cotangent,
    residual,
    norm_gain,
    route_ids,
    route_weights,
    expert_gate,
    expert_up,
    expert_down,
    out_proj,
    conv_out,
    branch_gate,
    prev_state,
    decay_param,
    rate_map,
    input_map,
):
    tok_rows, model_width = residual.shape
    sp_count = lax.axis_size("sp")
    tp_count = lax.axis_size("tp")
    experts_all = expert_gate.shape[0] * sp_count
    capacity = 4 * tok_rows // experts_all
    slot_total = experts_all * capacity
    block_rows = slot_total // sp_count
    channels = conv_out.shape[1]
    block_of = jnp.arange(channels, dtype=jnp.int32) // rate_map.shape[1]

    def whole_map(blocks):
        rows = blocks.reshape(channels, blocks.shape[2])
        tiled = jnp.tile(rows, (1, blocks.shape[0]))
        return jnp.where(block_of[:, None] == block_of[None, :], tiled, jnp.zeros((), tiled.dtype))

    maps = jnp.concatenate([whole_map(rate_map), whole_map(input_map)], axis=1)
    gain_row = norm_gain[None, :]
    soft_decay = jax.nn.softplus(-decay_param)[None, :]
    rows_in, cot_in, branch_out, *factors = dispatch(
        sp_count,
        tp_count,
        block_rows,
        (
            residual,
            cotangent,
            gain_row,
            route_ids,
            route_weights,
            conv_out,
            branch_gate,
            prev_state,
            soft_decay,
            maps,
        ),
        1,
    )
    rows_in = rows_in.reshape(slot_total, model_width)
    cot_in = cot_in.reshape(slot_total, model_width)
    gate_w, up_w, down_w = expert_gate[0], expert_up[0], expert_down[0]
    gate_pre = jnp.dot(rows_in, gate_w, preferred_element_type=jnp.float32)
    up_pre = jnp.dot(rows_in, up_w, preferred_element_type=jnp.float32)
    gate_sig = jax.nn.sigmoid(gate_pre)
    gate_act = gate_pre * gate_sig
    hidden = (gate_act * up_pre).astype(jnp.bfloat16)
    d_hidden = jnp.einsum("rd,fd->rf", cot_in, down_w, preferred_element_type=jnp.float32)
    d_up = (d_hidden * gate_act).astype(jnp.bfloat16)
    d_gate = (d_hidden * up_pre * gate_sig * (1.0 + gate_pre * (1.0 - gate_sig))).astype(
        jnp.bfloat16
    )
    grad_down = jnp.einsum("rf,rd->fd", hidden, cot_in, preferred_element_type=jnp.float32)[None]
    grad_gate = jnp.einsum("rd,rf->df", rows_in, d_gate, preferred_element_type=jnp.float32)[None]
    grad_up = jnp.einsum("rd,rf->df", rows_in, d_up, preferred_element_type=jnp.float32)[None]
    back_terms = jnp.einsum("rf,df->rd", d_gate, gate_w, preferred_element_type=jnp.float32)
    back_terms = back_terms + jnp.einsum("rf,df->rd", d_up, up_w, preferred_element_type=jnp.float32)
    back_terms = back_terms.astype(jnp.bfloat16).reshape(sp_count, block_rows, model_width)
    expert_hits = (
        route_ids[:, :, None] == jnp.arange(experts_all, dtype=jnp.int32)[None, None, :]
    ).astype(jnp.float32)
    token = jnp.arange(tok_rows, dtype=jnp.int32)
    earlier = (token[:, None] > token[None, :]).astype(jnp.bfloat16)
    ranks = jnp.dot(
        earlier,
        jnp.sum(expert_hits, axis=1).astype(jnp.bfloat16),
        preferred_element_type=jnp.float32,
    )
    slot_pair = route_ids * capacity + jnp.sum(ranks[:, None, :] * expert_hits, axis=2).astype(
        jnp.int32
    )
    slots = jnp.arange(slot_total, dtype=jnp.int32)
    slot_grid = slots.reshape(sp_count, 1, block_rows)
    pick = (
        (slot_grid == slot_pair[None, :, 0:1]) | (slot_grid == slot_pair[None, :, 1:2])
    ).astype(jnp.bfloat16)
    d_normed, branch_all = give_back(sp_count, tp_count, back_terms, pick, branch_out, 2)
    mix_cols, grad_conv_out, grad_branch_gate = tail(
        sp_count,
        tp_count,
        (d_normed, residual, cotangent, gain_row, out_proj, maps, *factors),
        3,
    )
    grad_out_proj = lax.dot_general(
        mix_cols.reshape(sp_count * tok_rows, mix_cols.shape[2]),
        branch_all.reshape(sp_count * tok_rows, channels),
        (((0,), (0,)), ((), ())),
        preferred_element_type=jnp.float32,
    )
    return (grad_gate, grad_up, grad_down, grad_out_proj, grad_conv_out, grad_branch_gate)


def solution(mesh):
    in_specs = (
        P("sp", None),
        P("sp", None),
        P(),
        P("sp", None),
        P("sp", None),
        P("sp", None, "tp"),
        P("sp", None, "tp"),
        P("sp", "tp", None),
        P(None, "tp"),
        P("sp", "tp"),
        P("sp", "tp"),
        P("sp", "tp"),
        P("tp"),
        P("tp", None, None),
        P("tp", None, None),
    )
    out_specs = (
        P("sp", None, "tp"),
        P("sp", None, "tp"),
        P("sp", "tp", None),
        P("sp", "tp"),
        P("sp", "tp"),
        P("sp", "tp"),
    )
    return jax.shard_map(
        per_device, mesh=mesh, in_specs=in_specs, out_specs=out_specs, check_vma=False
    )
```

```python
import functools

import jax
import jax.numpy as jnp
from jax import lax
from jax.sharding import PartitionSpec as P
from jax.experimental import pallas as pl
from jax.experimental.pallas import tpu as pltpu

RATE_SCALE = 8.0
NORM_EPS = 1e-06
SERIES_EDGE = 0.001
MESH = pl.DeviceIdType.MESH


def my_place(tp_count):
    s = lax.axis_index("sp")
    t = lax.axis_index("tp")
    beside = t + 1 - 2 * lax.rem(t, 2)
    across = lax.rem(t + tp_count // 2, tp_count)
    return s, t, beside, across


def hail(sp_count, s, t, beside, across):
    barrier = pltpu.get_barrier_semaphore()
    for other in (beside, across):
        pl.semaphore_signal(barrier, inc=1, device_id=(s, other), device_id_type=MESH)

    def one(i, carry):
        pl.semaphore_signal(
            barrier, inc=1, device_id=(lax.rem(s + i, sp_count), t), device_id_type=MESH
        )
        return carry

    lax.fori_loop(1, sp_count, one, 0)


def await_hails(sp_count):
    pl.semaphore_wait(pltpu.get_barrier_semaphore(), sp_count + 1)


def greet(sp_count, s, t, beside, across):
    hail(sp_count, s, t, beside, across)
    await_hails(sp_count)


def remote(src, dst, send_sem, recv_sem, device):
    return pltpu.make_async_remote_copy(
        src_ref=src,
        dst_ref=dst,
        send_sem=send_sem,
        recv_sem=recv_sem,
        device_id=device,
        device_id_type=MESH,
    )


def spreading(sp_count, tp_count, sends, outs, by_cols, local_sem, send_sem, recv_sem):
    s, t, beside, across = my_place(tp_count)
    facing = lax.rem(beside + tp_count // 2, tp_count)
    count = len(sends)

    def view(a, source, q):
        rows, cols = sends[a].shape[1:]
        if by_cols:
            return outs[a].at[source, :, pl.ds(pl.multiple_of(q * cols, cols), cols)]
        return outs[a].at[source, pl.ds(pl.multiple_of(q * rows, rows), rows), :]

    def first(a, i):
        target = lax.rem(s + i, sp_count)
        return remote(
            sends[a].at[target],
            view(a, s, t),
            send_sem.at[0, a, i],
            recv_sem.at[0, a, i],
            (target, t),
        )

    def own(a):
        return pltpu.make_async_copy(sends[a].at[s], view(a, s, t), local_sem.at[a])

    def passed(kind, a, i, q, to):
        source = lax.rem(s + sp_count - i, sp_count)
        block = view(a, source, q)
        return remote(block, block, send_sem.at[kind, a, i], recv_sem.at[kind, a, i], (s, to))

    def pass_on(i):
        for a in range(count):
            passed(1, a, i, t, across).start()
            passed(2, a, i, t, beside).start()

    def pass_back(i):
        for a in range(count):
            passed(1, a, i, across, across).wait_recv()
            passed(3, a, i, across, beside).start()

    def landed(i):
        for a in range(count):
            source = lax.rem(s + sp_count - i, sp_count)
            remote(
                sends[a].at[source],
                view(a, source, t),
                send_sem.at[0, a, i],
                recv_sem.at[0, a, i],
                (source, t),
            ).wait_recv()

    def start(i):
        for a in range(count):
            first(a, i).start()

    def start_own():
        for a in range(count):
            own(a).start()

    def pass_own():
        for a in range(count):
            own(a).wait()
        pass_on(0)

    def relay():
        landed(1)
        pass_on(1)

        def middle(i, carry):
            landed(i)
            pass_on(i)
            pass_back(i - 2)
            return carry

        lax.fori_loop(2, sp_count, middle, 0)
        pass_back(sp_count - 2)
        pass_back(sp_count - 1)

    def finish():
        def one(i, carry):
            for a in range(count):
                passed(2, a, i, beside, beside).wait_recv()
                passed(3, a, i, facing, beside).wait_recv()
                passed(1, a, i, t, across).wait_send()
                passed(2, a, i, t, beside).wait_send()
                passed(3, a, i, across, beside).wait_send()
            return carry

        lax.fori_loop(0, sp_count, one, 0)

        def one_first(i, carry):
            for a in range(count):
                first(a, i).wait_send()
            return carry

        lax.fori_loop(1, sp_count, one_first, 0)

    def complete(i):
        for a in range(count):
            passed(2, a, i, beside, beside).wait_recv()
            passed(3, a, i, facing, beside).wait_recv()

    def finish_sends():
        def one(i, carry):
            for a in range(count):
                passed(1, a, i, t, across).wait_send()
                passed(2, a, i, t, beside).wait_send()
                passed(3, a, i, across, beside).wait_send()
            return carry

        lax.fori_loop(0, sp_count, one, 0)

        def one_first(i, carry):
            for a in range(count):
                first(a, i).wait_send()
            return carry

        lax.fori_loop(1, sp_count, one_first, 0)

    steps = (landed, pass_on, pass_back, complete, finish_sends)
    return start, start_own, pass_own, relay, finish, steps


def spread_sems(sp_count, count):
    return [
        pltpu.SemaphoreType.DMA((count,)),
        pltpu.SemaphoreType.DMA((4, count, sp_count)),
        pltpu.SemaphoreType.DMA((4, count, sp_count)),
    ]


def one_less_exp(spread):
    small = jnp.minimum(spread, 0.3)
    series = jnp.full_like(small, 1.0 / 40320.0)
    for factorial in (5040.0, 720.0, 120.0, 24.0, 6.0, 2.0, 1.0):
        series = 1.0 / factorial - small * series
    return jnp.where(spread < 0.3, small * series, 1.0 - jnp.exp(-spread))


def dispatch_kernel(
    sp_count,
    tp_count,
    res,
    cot,
    gain,
    ids,
    weights,
    conv,
    gate,
    prev,
    soft,
    maps,
    gate_w,
    up_w,
    down_w,
    rows_out,
    cot_out,
    full,
    branch_all,
    hidden_out,
    d_gate_out,
    d_up_out,
    rate_factor,
    input_factor,
    direct_factor,
    gate_factor,
    gelu_out,
    keep_out,
    send_rows,
    send_cot,
    moe_part,
    scaled_first,
    scaled_second,
    pre_values,
    rows_held,
    cot_held,
    branch_out,
    part,
    from_beside,
    to_across,
    from_across,
    mine,
    leaving,
    arrived,
    quarter,
    local_sem,
    send_sem,
    recv_sem,
    back_send,
    back_recv,
    branch_send,
    branch_recv,
    last_send,
    last_recv,
    keep_sem,
    own_sem,
):
    s, t, beside, across = my_place(tp_count)
    hail(sp_count, s, t, beside, across)
    start, start_own, pass_own, relay, finish, steps = spreading(
        sp_count,
        tp_count,
        (send_rows, send_cot),
        (rows_held, cot_held),
        True,
        local_sem,
        send_sem,
        recv_sem,
    )
    tok_rows = res.shape[0]
    cap, width = send_rows.shape[1:]
    cols = pl.ds(pl.multiple_of(t * width, width), width)
    res_all = res[...].astype(jnp.float32)
    inv_rms = lax.rsqrt(jnp.mean(res_all * res_all, axis=1, keepdims=True) + NORM_EPS)
    moe_part[...] = (res[:, cols].astype(jnp.float32) * inv_rms * gain[:, cols]).astype(
        jnp.bfloat16
    )
    cot_mine = cot[:, cols].astype(jnp.float32)
    scaled_first[...] = (weights[:, 0:1] * cot_mine).astype(jnp.bfloat16)
    scaled_second[...] = (weights[:, 1:2] * cot_mine).astype(jnp.bfloat16)
    experts = lax.broadcasted_iota(jnp.int32, (tok_rows, sp_count), 1)
    is_first = ids[:, 0:1] == experts
    is_second = ids[:, 1:2] == experts
    hits = (is_first | is_second).astype(jnp.float32).astype(jnp.bfloat16)
    earlier = (
        lax.broadcasted_iota(jnp.int32, (tok_rows, tok_rows), 0)
        > lax.broadcasted_iota(jnp.int32, (tok_rows, tok_rows), 1)
    )
    earlier = earlier.astype(jnp.float32).astype(jnp.bfloat16)
    ranks = jnp.dot(earlier, hits, preferred_element_type=jnp.float32)
    slot_first = jnp.sum(jnp.where(is_first, ranks, 0.0), axis=1, keepdims=True)
    slot_second = jnp.sum(jnp.where(is_second, ranks, 0.0), axis=1, keepdims=True)
    slot_first = slot_first + (ids[:, 0:1] * cap).astype(jnp.float32)
    slot_second = slot_second + (ids[:, 1:2] * cap).astype(jnp.float32)
    lanes = lax.broadcasted_iota(jnp.int32, (tok_rows, cap), 1).astype(jnp.float32)
    over_rows = (((0,), (0,)), ((), ()))

    def fill(target):
        base = (target * cap).astype(jnp.float32)
        first = jnp.where(slot_first - base == lanes, 1.0, 0.0)
        second = jnp.where(slot_second - base == lanes, 1.0, 0.0)
        send_rows[target] = lax.dot_general(
            (first + second).astype(jnp.bfloat16),
            moe_part[...],
            over_rows,
            preferred_element_type=jnp.float32,
        ).astype(jnp.bfloat16)
        from_first = lax.dot_general(
            first.astype(jnp.bfloat16),
            scaled_first[...],
            over_rows,
            preferred_element_type=jnp.float32,
        )
        from_second = lax.dot_general(
            second.astype(jnp.bfloat16),
            scaled_second[...],
            over_rows,
            preferred_element_type=jnp.float32,
        )
        send_cot[target] = (from_first + from_second).astype(jnp.bfloat16)

    fill(s)
    await_hails(sp_count)
    start_own()

    def send_one(i, carry):
        fill(lax.rem(s + i, sp_count))
        start(i)
        return carry

    lax.fori_loop(1, sp_count, send_one, 0)
    pass_own()
    channels = conv.shape[1]
    pre_values[...] = jnp.dot(conv[...], maps[...], preferred_element_type=jnp.float32)
    step = 16

    def forward(i, carry):
        rows = pl.ds(pl.multiple_of(i * step, step), step)
        rate_gate = jax.nn.sigmoid(pre_values[rows, :channels])
        input_gate = jax.nn.sigmoid(pre_values[rows, channels:])
        log_keep = -RATE_SCALE * rate_gate * soft[...]
        keep = jnp.exp(log_keep)
        spread = -2.0 * log_keep
        gone = one_less_exp(spread)
        norm_term = jnp.sqrt(gone)
        conv_values = conv[rows, :].astype(jnp.float32)
        prev_values = prev[rows, :].astype(jnp.float32)
        inner = input_gate * conv_values
        state_now = keep * prev_values + norm_term * inner
        v = gate[rows, :].astype(jnp.float32)
        root = 0.7978845608028654
        bent = jnp.tanh(root * (v + 0.044715 * v * v * v))
        gelu_value = 0.5 * v * (1.0 + bent)
        gelu_slope = 0.5 * (1.0 + bent) + 0.5 * v * (1.0 - bent * bent) * root * (
            1.0 + 3.0 * 0.044715 * v * v
        )
        tiny_side = spread < SERIES_EDGE
        series = jnp.where(tiny_side, 1.0 + 0.5 * spread, spread / jnp.where(tiny_side, 1.0, gone))
        slope = 0.5 * jnp.sqrt(spread * series)
        branch_out[rows, :] = (state_now * gelu_value).astype(jnp.bfloat16)
        rate_factor[rows, :] = prev_values * keep * (
            -RATE_SCALE * soft[...]
        ) * rate_gate * (1.0 - rate_gate) + inner * keep * keep * (1.0 - rate_gate) * slope
        input_factor[rows, :] = norm_term * conv_values * input_gate * (1.0 - input_gate)
        direct_factor[rows, :] = norm_term * input_gate
        gate_factor[rows, :] = state_now * gelu_slope
        gelu_out[rows, :] = gelu_value
        keep_out[rows, :] = keep
        return carry

    lax.fori_loop(0, tok_rows // step, forward, 0)
    landed, pass_on, pass_back, complete, finish_sends = steps
    facing = lax.rem(beside + tp_count // 2, tp_count)
    half = sp_count // 2
    s_twin = s + 1 - 2 * lax.rem(s, 2)
    over_cols = (((1,), (1,)), ((), ()))

    def cols_of(q):
        return pl.ds(pl.multiple_of(q * width, width), width)

    def source_of(i):
        return lax.rem(s + sp_count - i, sp_count)

    def branch_copy(j):
        return remote(
            branch_out,
            branch_all.at[s],
            branch_send.at[0, j],
            branch_recv.at[0, j],
            (lax.rem(s + 2 * j, sp_count), t),
        )

    def branch_twin(j):
        block = branch_all.at[lax.rem(s + sp_count - 2 * j, sp_count)]
        return remote(block, block, branch_send.at[1, j], branch_recv.at[1, j], (s_twin, t))

    own_branch = pltpu.make_async_copy(branch_out, branch_all.at[s], own_sem.at[0])
    own_branch.start()

    def start_branch(j, carry):
        branch_copy(j).start()
        return carry

    lax.fori_loop(1, half, start_branch, 0)

    def kept(i):
        source = source_of(i)
        return (
            pltpu.make_async_copy(rows_held.at[source], rows_out.at[source], keep_sem.at[0, i]),
            pltpu.make_async_copy(cot_held.at[source], cot_out.at[source], keep_sem.at[1, i]),
        )

    def to_beside(i, k):
        q = beside if k == 0 else facing
        return remote(
            part.at[source_of(i), :, cols_of(q)],
            from_beside.at[k, source_of(i)],
            back_send.at[k, i],
            back_recv.at[k, i],
            (s, beside),
        )

    def crossing(i):
        return remote(
            to_across.at[source_of(i)],
            from_across.at[source_of(i)],
            back_send.at[2, i],
            back_recv.at[2, i],
            (s, across),
        )

    def homeward(i):
        return remote(
            leaving.at[source_of(i)],
            arrived.at[s],
            back_send.at[3, i],
            back_recv.at[3, i],
            (source_of(i), t),
        )

    def expert(i):
        complete(i)
        for copy in kept(i):
            copy.start()
        source = source_of(i)
        rows_in = rows_held[source]
        gate_pre = jnp.dot(rows_in, gate_w[...], preferred_element_type=jnp.float32)
        up_pre = jnp.dot(rows_in, up_w[...], preferred_element_type=jnp.float32)
        d_hidden = lax.dot_general(
            cot_held[source], down_w[...], over_cols, preferred_element_type=jnp.float32
        )
        gate_sig = jax.nn.sigmoid(gate_pre)
        gate_act = gate_pre * gate_sig
        d_up = (d_hidden * gate_act).astype(jnp.bfloat16)
        d_gate = (d_hidden * up_pre * gate_sig * (1.0 + gate_pre * (1.0 - gate_sig))).astype(
            jnp.bfloat16
        )
        hidden_out[source] = (gate_act * up_pre).astype(jnp.bfloat16)
        d_up_out[source] = d_up
        d_gate_out[source] = d_gate
        back = lax.dot_general(d_gate, gate_w[...], over_cols, preferred_element_type=jnp.float32)
        back = back + lax.dot_general(
            d_up, up_w[...], over_cols, preferred_element_type=jnp.float32
        )
        part[source] = back.astype(jnp.bfloat16)
        to_beside(i, 1).start()
        to_beside(i, 0).start()

    def cross(i):
        to_beside(i, 1).wait_recv()
        at = source_of(i)
        total = part[at, :, cols_of(across)].astype(jnp.float32) + from_beside[1, at].astype(
            jnp.float32
        )
        to_across[at] = total.astype(jnp.bfloat16)
        crossing(i).start()
        to_beside(i, 0).wait_recv()
        mine[at] = part[at, :, cols_of(t)].astype(jnp.float32) + from_beside[0, at].astype(
            jnp.float32
        )

    def leave(i):
        crossing(i).wait_recv()
        at = source_of(i)
        total = (mine[at] + from_across[at].astype(jnp.float32)).astype(jnp.bfloat16)

        @pl.when(i > 0)
        def _():
            leaving[at] = total
            homeward(i).start()

        @pl.when(i == 0)
        def _():
            arrived[s] = total

    def turn(i, carry):
        @pl.when((i >= 1) & (i < sp_count))
        def _():
            landed(i)
            pass_on(i)

        @pl.when((i >= 1) & (i < sp_count + 1))
        def _():
            pass_back(i - 1)

        @pl.when((i >= 2) & (i < sp_count + 2))
        def _():
            expert(i - 2)

        @pl.when((i >= 3) & (i < sp_count + 3))
        def _():
            cross(i - 3)

        @pl.when(i >= 4)
        def _():
            leave(i - 4)

        return carry

    lax.fori_loop(0, sp_count + 4, turn, 0)
    own_branch.wait()
    branch_twin(0).start()

    def pass_branch(j, carry):
        branch_copy(j).wait_recv()
        branch_twin(j).start()
        return carry

    lax.fori_loop(1, half, pass_branch, 0)

    def gather_rows(source):
        base = (source * cap).astype(jnp.float32)
        chosen = jnp.where(slot_first - base == lanes, 1.0, 0.0)
        chosen = chosen + jnp.where(slot_second - base == lanes, 1.0, 0.0)
        return jnp.dot(
            chosen.astype(jnp.bfloat16), arrived[source], preferred_element_type=jnp.float32
        )

    def add_in(i, total):
        source = lax.rem(s + i, sp_count)
        remote(
            leaving.at[source],
            arrived.at[source],
            back_send.at[3, i],
            back_recv.at[3, i],
            (source, t),
        ).wait_recv()
        return total + gather_rows(source)

    quarter[...] = lax.fori_loop(1, sp_count, add_in, gather_rows(s)).astype(jnp.bfloat16)

    def gathered(kind, source, q, to):
        return remote(
            source, full.at[:, cols_of(q)], last_send.at[kind], last_recv.at[kind], (s, to)
        )

    own_quarter = pltpu.make_async_copy(quarter, full.at[:, cols_of(t)], own_sem.at[1])
    gathered(0, quarter, t, across).start()
    gathered(1, quarter, t, beside).start()
    own_quarter.start()
    gathered(0, quarter, across, across).wait_recv()
    gathered(2, full.at[:, cols_of(across)], across, beside).start()
    finish_sends()

    def end(i, carry):
        to_beside(i, 0).wait_send()
        to_beside(i, 1).wait_send()
        crossing(i).wait_send()
        for copy in kept(i):
            copy.wait()
        return carry

    lax.fori_loop(0, sp_count, end, 0)

    def end_home(i, carry):
        homeward(i).wait_send()
        return carry

    lax.fori_loop(1, sp_count, end_home, 0)

    def end_branch(j, carry):
        branch_copy(j).wait_send()
        branch_twin(j).wait()
        return carry

    lax.fori_loop(1, half, end_branch, 0)
    branch_twin(0).wait()
    own_quarter.wait()
    gathered(1, quarter, beside, beside).wait_recv()
    gathered(2, full.at[:, cols_of(facing)], facing, beside).wait_recv()
    gathered(0, quarter, t, across).wait_send()
    gathered(1, quarter, t, beside).wait_send()
    gathered(2, full.at[:, cols_of(across)], across, beside).wait_send()


def dispatch(sp_count, tp_count, cap, operands, number):
    res, conv = operands[0], operands[5]
    tok_rows, model_width = res.shape
    width = model_width // tp_count
    wide = jax.ShapeDtypeStruct((sp_count, cap, model_width), jnp.bfloat16)
    units = jax.ShapeDtypeStruct((sp_count, cap, operands[-1].shape[0]), jnp.bfloat16)
    factor = jax.ShapeDtypeStruct(conv.shape, jnp.float32)
    blocks = (sp_count, cap, width)
    vmem = pl.BlockSpec(memory_space=pltpu.VMEM)
    anywhere = pl.BlockSpec(memory_space=pl.ANY)
    return pl.pallas_call(
        functools.partial(dispatch_kernel, sp_count, tp_count),
        out_shape=[
            wide,
            wide,
            jax.ShapeDtypeStruct(res.shape, jnp.bfloat16),
            jax.ShapeDtypeStruct((sp_count,) + conv.shape, jnp.bfloat16),
        ]
        + [units] * 3
        + [factor] * 6,
        in_specs=[vmem] * len(operands),
        out_specs=[anywhere] * 4 + [vmem] * 9,
        scratch_shapes=[
            pltpu.VMEM((sp_count, cap, width), jnp.bfloat16),
            pltpu.VMEM((sp_count, cap, width), jnp.bfloat16),
            pltpu.VMEM((tok_rows, width), jnp.bfloat16),
            pltpu.VMEM((tok_rows, width), jnp.bfloat16),
            pltpu.VMEM((tok_rows, width), jnp.bfloat16),
            pltpu.VMEM((tok_rows, 2 * conv.shape[1]), jnp.float32),
            pltpu.VMEM((sp_count, cap, model_width), jnp.bfloat16),
            pltpu.VMEM((sp_count, cap, model_width), jnp.bfloat16),
            pltpu.VMEM(conv.shape, jnp.bfloat16),
            pltpu.VMEM((sp_count, cap, model_width), jnp.bfloat16),
            pltpu.VMEM((2,) + blocks, jnp.bfloat16),
            pltpu.VMEM(blocks, jnp.bfloat16),
            pltpu.VMEM(blocks, jnp.bfloat16),
            pltpu.VMEM(blocks, jnp.float32),
            pltpu.VMEM(blocks, jnp.bfloat16),
            pltpu.VMEM(blocks, jnp.bfloat16),
            pltpu.VMEM((tok_rows, width), jnp.bfloat16),
        ]
        + spread_sems(sp_count, 2)
        + [
            pltpu.SemaphoreType.DMA((4, sp_count)),
            pltpu.SemaphoreType.DMA((4, sp_count)),
            pltpu.SemaphoreType.DMA((2, sp_count // 2)),
            pltpu.SemaphoreType.DMA((2, sp_count // 2)),
            pltpu.SemaphoreType.DMA((3,)),
            pltpu.SemaphoreType.DMA((3,)),
            pltpu.SemaphoreType.DMA((2, sp_count)),
            pltpu.SemaphoreType.DMA((2,)),
        ],
        compiler_params=pltpu.CompilerParams(collective_id=number, has_side_effects=True),
        cost_estimate=pl.CostEstimate(flops=0, bytes_accessed=40_000_000, transcendentals=0),
    )(*operands)


def tail_kernel(
    sp_count,
    tp_count,
    normed,
    res,
    cot,
    gain,
    proj,
    maps,
    rate_factor,
    input_factor,
    direct_factor,
    gate_factor,
    gelu_values,
    keep,
    mix_out,
    conv_grad,
    gate_grad,
    share,
    mix,
    small,
    small_all,
    local_sem,
    send_sem,
    recv_sem,
    small_send,
    small_recv,
):
    s, t, beside, across = my_place(tp_count)
    hail(sp_count, s, t, beside, across)
    start, start_own, pass_own, relay, finish, steps = spreading(
        sp_count, tp_count, (share,), (mix_out,), False, local_sem, send_sem, recv_sem
    )
    tok_rows, model_width = res.shape
    share_rows, out_rows = share.shape[1:]

    def mix_rows(begin):
        rows = pl.ds(pl.multiple_of(begin, share_rows), share_rows)
        values = res[rows, :].astype(jnp.float32)
        weighted = gain[...] * normed[rows, :].astype(jnp.float32)
        inv_rms = lax.rsqrt(jnp.mean(values * values, axis=1, keepdims=True) + NORM_EPS)
        cubed = inv_rms * inv_rms * inv_rms
        slope = cubed * jnp.mean(values * weighted, axis=1, keepdims=True)
        return rows, (
            cot[rows, :].astype(jnp.float32) + inv_rms * weighted - values * slope
        ).astype(jnp.bfloat16)

    _, own_rows = mix_rows(t * share_rows)
    for j in range(sp_count):
        share[j] = own_rows[:, j * out_rows : (j + 1) * out_rows]
    await_hails(sp_count)
    start_own()

    def send_one(i, carry):
        start(i)
        return carry

    lax.fori_loop(1, sp_count, send_one, 0)

    def fill(k, carry):
        rows, values = mix_rows(k * share_rows)
        mix[rows, :] = values
        return carry

    lax.fori_loop(0, tp_count, fill, 0)
    pass_own()
    d_branch = jnp.dot(mix[...], proj[...], preferred_element_type=jnp.float32)
    gate_grad[...] = d_branch * gate_factor[...]
    at = lax.broadcasted_iota(jnp.int32, d_branch.shape, 0)
    grads = d_branch * gelu_values[...]
    keeps = jnp.where(at < tok_rows - 1, pltpu.roll(keep[...], tok_rows - 1, 0), 1.0)
    reach = 1
    while reach < tok_rows:
        inside = at < tok_rows - reach
        later_grads = jnp.where(inside, pltpu.roll(grads, tok_rows - reach, 0), 0.0)
        later_keeps = jnp.where(inside, pltpu.roll(keeps, tok_rows - reach, 0), 1.0)
        grads = grads + keeps * later_grads
        keeps = keeps * later_keeps
        reach *= 2
    small[...] = jnp.zeros_like(small)
    small[0:1, :] = keep[0:1, :] * keeps[0:1, :]
    small[1:2, :] = keep[0:1, :] * grads[0:1, :]
    small_all[s] = jnp.zeros(small.shape, jnp.float32)

    def carry_to(i):
        return remote(
            small,
            small_all.at[s],
            small_send.at[i],
            small_recv.at[i],
            (lax.rem(s + i, sp_count), t),
        )

    def send_small(i, carry):
        carry_to(i).start()
        return carry

    lax.fori_loop(1, sp_count, send_small, 0)
    relay()

    def take_small(i, carry):
        source = lax.rem(s + sp_count - i, sp_count)
        remote(
            small, small_all.at[source], small_send.at[i], small_recv.at[i], (source, t)
        ).wait_recv()
        return carry

    lax.fori_loop(1, sp_count, take_small, 0)

    def compose(turn, carried):
        source = sp_count - 1 - turn
        later = small_all[source]
        return jnp.where(source > s, later[1:2] + later[0:1] * carried, carried)

    carried = lax.fori_loop(
        0, sp_count - 1, compose, jnp.zeros((1, d_branch.shape[1]), jnp.float32)
    )
    state_grad = grads + keeps * carried
    back = jnp.concatenate(
        [state_grad * rate_factor[...], state_grad * input_factor[...]], axis=1
    )
    high = back.astype(jnp.bfloat16)
    low = (back - high.astype(jnp.float32)).astype(jnp.bfloat16)
    over_cols = (((1,), (1,)), ((), ()))
    conv_grad[...] = (
        state_grad * direct_factor[...]
        + lax.dot_general(high, maps[...], over_cols, preferred_element_type=jnp.float32)
        + lax.dot_general(low, maps[...], over_cols, preferred_element_type=jnp.float32)
    )
    finish()

    def end_small(i, carry):
        carry_to(i).wait_send()
        return carry

    lax.fori_loop(1, sp_count, end_small, 0)


def tail(sp_count, tp_count, operands, number):
    res, keep = operands[1], operands[-1]
    tok_rows, model_width = res.shape
    share_rows, out_rows = tok_rows // tp_count, model_width // sp_count
    factor = jax.ShapeDtypeStruct(keep.shape, jnp.float32)
    vmem = pl.BlockSpec(memory_space=pltpu.VMEM)
    return pl.pallas_call(
        functools.partial(tail_kernel, sp_count, tp_count),
        out_shape=[
            jax.ShapeDtypeStruct((sp_count, tok_rows, out_rows), jnp.bfloat16),
            factor,
            factor,
        ],
        in_specs=[vmem] * len(operands),
        out_specs=[pl.BlockSpec(memory_space=pl.ANY), vmem, vmem],
        scratch_shapes=[
            pltpu.VMEM((sp_count, share_rows, out_rows), jnp.bfloat16),
            pltpu.VMEM((tok_rows, model_width), jnp.bfloat16),
            pltpu.VMEM((8, keep.shape[1]), jnp.float32),
            pltpu.VMEM((sp_count, 8, keep.shape[1]), jnp.float32),
        ]
        + spread_sems(sp_count, 1)
        + [pltpu.SemaphoreType.DMA((sp_count,)), pltpu.SemaphoreType.DMA((sp_count,))],
        compiler_params=pltpu.CompilerParams(collective_id=number, has_side_effects=True),
        cost_estimate=pl.CostEstimate(flops=0, bytes_accessed=20_000_000, transcendentals=0),
    )(*operands)


def per_device(
    cotangent,
    residual,
    norm_gain,
    route_ids,
    route_weights,
    expert_gate,
    expert_up,
    expert_down,
    out_proj,
    conv_out,
    branch_gate,
    prev_state,
    decay_param,
    rate_map,
    input_map,
):
    tok_rows, model_width = residual.shape
    sp_count = lax.axis_size("sp")
    tp_count = lax.axis_size("tp")
    experts_all = expert_gate.shape[0] * sp_count
    capacity = 4 * tok_rows // experts_all
    slot_total = experts_all * capacity
    block_rows = slot_total // sp_count
    channels = conv_out.shape[1]
    block_of = jnp.arange(channels, dtype=jnp.int32) // rate_map.shape[1]

    def whole_map(blocks):
        rows = blocks.reshape(channels, blocks.shape[2])
        tiled = jnp.tile(rows, (1, blocks.shape[0]))
        return jnp.where(block_of[:, None] == block_of[None, :], tiled, jnp.zeros((), tiled.dtype))

    maps = jnp.concatenate([whole_map(rate_map), whole_map(input_map)], axis=1)
    gain_row = norm_gain[None, :]
    soft_decay = jax.nn.softplus(-decay_param)[None, :]
    rows_in, cot_in, d_normed, branch_all, hidden, d_gate, d_up, *factors = dispatch(
        sp_count,
        tp_count,
        block_rows,
        (
            residual,
            cotangent,
            gain_row,
            route_ids,
            route_weights,
            conv_out,
            branch_gate,
            prev_state,
            soft_decay,
            maps,
            expert_gate[0],
            expert_up[0],
            expert_down[0],
        ),
        1,
    )
    rows_in = rows_in.reshape(slot_total, model_width)
    cot_in = cot_in.reshape(slot_total, model_width)
    hidden = hidden.reshape(slot_total, hidden.shape[2])
    d_gate = d_gate.reshape(hidden.shape)
    d_up = d_up.reshape(hidden.shape)
    grad_down = jnp.einsum("rf,rd->fd", hidden, cot_in, preferred_element_type=jnp.float32)[None]
    grad_gate = jnp.einsum("rd,rf->df", rows_in, d_gate, preferred_element_type=jnp.float32)[None]
    grad_up = jnp.einsum("rd,rf->df", rows_in, d_up, preferred_element_type=jnp.float32)[None]
    mix_cols, grad_conv_out, grad_branch_gate = tail(
        sp_count,
        tp_count,
        (d_normed, residual, cotangent, gain_row, out_proj, maps, *factors),
        3,
    )
    grad_out_proj = lax.dot_general(
        mix_cols.reshape(sp_count * tok_rows, mix_cols.shape[2]),
        branch_all.reshape(sp_count * tok_rows, channels),
        (((0,), (0,)), ((), ())),
        preferred_element_type=jnp.float32,
    )
    return (grad_gate, grad_up, grad_down, grad_out_proj, grad_conv_out, grad_branch_gate)


def solution(mesh):
    in_specs = (
        P("sp", None),
        P("sp", None),
        P(),
        P("sp", None),
        P("sp", None),
        P("sp", None, "tp"),
        P("sp", None, "tp"),
        P("sp", "tp", None),
        P(None, "tp"),
        P("sp", "tp"),
        P("sp", "tp"),
        P("sp", "tp"),
        P("tp"),
        P("tp", None, None),
        P("tp", None, None),
    )
    out_specs = (
        P("sp", None, "tp"),
        P("sp", None, "tp"),
        P("sp", "tp", None),
        P("sp", "tp"),
        P("sp", "tp"),
        P("sp", "tp"),
    )
    return jax.shard_map(
        per_device, mesh=mesh, in_specs=in_specs, out_specs=out_specs, check_vma=False
    )
```
